256 devices in a mesh: rep: 2 (over z_hi), fs: 16 (over z_lo, x), tp: 8 (over y, core).
Axes of the slice: x: 4, y: 4, z: 8 (z_hi: 2, z_lo: 4; z = z_hi * 4 + z_lo), core: 2. Of those that a mesh axis runs over, the one named last changes fastest.
Arguments:
- stream: bfloat16 [32768, 2048], P(('rep', 'fs', 'tp')), may hold values from -6 to 6
- gate_weight: bfloat16 [2048, 2816], P('fs', 'tp'), may hold values from -0.125 to 0.125
- up_weight: bfloat16 [2048, 2816], P('fs', 'tp'), may hold values from -0.125 to 0.125
- down_weight: bfloat16 [2816, 2048], P('tp', 'fs'), may hold values from -0.21875 to 0.21875
- query_weight: bfloat16 [2048, 512], P('fs', 'tp'), may hold values from -0.125 to 0.125
- key_weight: bfloat16 [2048, 512], P('fs', 'tp'), may hold values from -0.125 to 0.125
- value_weight: bfloat16 [2048, 1024], P('fs', 'tp'), may hold values from -0.125 to 0.125
- outgate_weight: bfloat16 [2048, 1024], P('fs', 'tp'), may hold values from -0.125 to 0.125
- decay_down: bfloat16 [2048, 32], replicated, may hold values from -0.125 to 0.125
- decay_up: bfloat16 [32, 512], P(None, 'tp'), may hold values from -2 to 2
- decay_bias: float32 [512], P('tp'), may hold values from -0.5 to 7
- head_gain: float32 [128], replicated, may hold values from 0.1 to 1.9
- out_weight: bfloat16 [1024, 2048], P('tp', 'fs'), may hold values from -0.375 to 0.375
- norm_gain: float32 [3, 2048], replicated, may hold values from 0.1 to 1.9
Outputs:
- layer_out: bfloat16 [32768, 2048], P(('rep', 'fs', 'tp'))
The draws below stay inside these ranges and needn't reach their ends.
All inputs are finite; a program needn't handle non-finite values.
Results may differ from the reference program's by a relative error of at most 0.015.
Values may be sent and summed in bfloat16 or wider, within the bound.
No kernel may reach another device: no remote copies, remote signals or barrier semaphores. Data moves between devices by JAX's collectives and lax.ppermute only.
A program may use at most 128 MiB of HBM per device.

```python
import jax
import jax.numpy as jnp
from jax import lax

D = 2048
FF = 2816
HEADS = 8
DK = 64
DV = 128
GR = 32
BLOCK = 64
KW = 512
VW = 1024
SEQLEN = 1024
SEQS = 32
TOKENS = 32768


def draw_decay_bias(key, part):
    pick_key, fast_key, slow_key = jax.random.split(key, 3)
    share = 0.5
    quick = jax.random.uniform(pick_key, (HEADS, 1), jnp.float32) < share
    fast_values = jax.random.uniform(fast_key, (HEADS, DK), jnp.float32, -0.5, 1.5)
    slow_values = jax.random.uniform(slow_key, (HEADS, DK), jnp.float32, 4.0, 7.0)
    return jnp.where(quick, fast_values, slow_values).reshape(HEADS * DK)


def shard_levels(rng, extent, cuts, least, top_value):
    gain, own = 1.0, jax.random.fold_in(rng, 6)
    for axis_at, parts in cuts:
        steps = jnp.exp(jax.random.uniform(jax.random.fold_in(own, axis_at), (parts,), jnp.float32, least / len(cuts), top_value / len(cuts)))
        gain = gain * jnp.repeat(steps, extent[axis_at] // parts).reshape([-1 if axis == axis_at else 1 for axis in range(len(extent))])
    return gain


def scatter_about(own_key, dims, width, reach, cuts=(), kind=jnp.bfloat16):
    entries = width * jax.random.normal(own_key, dims, jnp.float32)
    if cuts:
        entries = entries * shard_levels(own_key, dims, cuts, -0.22, 0.18)
    return jnp.clip(entries, -reach, reach).astype(kind)


def setup_inputs(seed: int = 0) -> dict:
    arg_keys = jax.random.split(jax.random.key(seed), 15)
    return {
        "stream": scatter_about(arg_keys[0], (TOKENS, D), 1.0, 6.0, ((0, 256),)),
        "gate_weight": scatter_about(arg_keys[1], (D, FF), D ** -0.5, 0.125, ((0, 16), (1, 8))),
        "up_weight": scatter_about(arg_keys[2], (D, FF), D ** -0.5, 0.125, ((0, 16), (1, 8))),
        "down_weight": scatter_about(arg_keys[3], (FF, D), (FF // 4) ** -0.5, 0.21875, ((0, 8), (1, 16))),
        "query_weight": scatter_about(arg_keys[4], (D, KW), D ** -0.5, 0.125, ((0, 16), (1, 8))),
        "key_weight": scatter_about(arg_keys[5], (D, KW), D ** -0.5, 0.125, ((0, 16), (1, 8))),
        "value_weight": scatter_about(arg_keys[6], (D, VW), D ** -0.5, 0.125, ((0, 16), (1, 8))),
        "outgate_weight": scatter_about(arg_keys[7], (D, VW), D ** -0.5, 0.125, ((0, 16), (1, 8))),
        "decay_down": scatter_about(arg_keys[8], (D, GR), D ** -0.5, 0.125),
        "decay_up": scatter_about(arg_keys[9], (GR, KW), (GR // 4) ** -0.5, 2.0, ((1, 8),)),
        "decay_bias": draw_decay_bias(jax.random.fold_in(arg_keys[14], 71), 0),
        "head_gain": jnp.clip(1.0 + 0.18 * jax.random.normal(arg_keys[11], (DV,), jnp.float32), 0.1, 1.9),
        "out_weight": scatter_about(arg_keys[12], (VW, D), (VW // 4) ** -0.5, 0.375, ((0, 8), (1, 16))),
        "norm_gain": jnp.clip(1.0 + 0.18 * jax.random.normal(arg_keys[13], (3, D), jnp.float32), 0.1, 1.9),
    }


RESIDUAL_SCALE = 2.0 ** 0.5
BRANCH_SCALE = 0.5
NORM_EPS = 1e-05
HEAD_EPS = 0.01
GATE_DIVISOR = 16.0

def layer_norm(values, norm_scale):
    average = lax.optimization_barrier(jnp.mean(values, -1, keepdims=True))
    centred = values - average
    spread = lax.optimization_barrier(jnp.mean(centred * centred, -1, keepdims=True))
    return (centred * lax.rsqrt(spread + NORM_EPS) * norm_scale).astype(jnp.bfloat16)

def blocked_mixer(query, key_rows, value_rows, log_gate):
    length, head_count, key_dim = query.shape
    value_dim = value_rows.shape[2]
    block_count = length // BLOCK
    highest = lax.Precision.HIGHEST

    def split_blocks(values):
        return values.reshape(block_count, BLOCK, head_count, values.shape[2]).transpose(0, 2, 1, 3)
    causal = jnp.tril(jnp.ones((BLOCK, BLOCK), dtype=bool))

    def advance(carried, inputs):
        query_blk, key_blk, value_blk, decay_blk = inputs
        log_gaps = decay_blk[:, :, None, :] - decay_blk[:, None, :, :]
        log_gaps = jnp.where(causal[None, :, :, None], log_gaps, -jnp.inf)
        scores = lax.optimization_barrier(jnp.sum(query_blk[:, :, None, :] * key_blk[:, None, :, :] * jnp.exp(log_gaps), axis=-1))
        inside = jnp.einsum('hij,hjv->hiv', scores, value_blk, precision=highest)
        carried_part = jnp.einsum('hid,hdv->hiv', query_blk * jnp.exp(decay_blk), carried, precision=highest)
        closing = decay_blk[:, -1, :]
        update = jnp.einsum('hjd,hjv->hdv', key_blk * jnp.exp(closing[:, None, :] - decay_blk), value_blk, precision=highest)
        return (carried * jnp.exp(closing)[:, :, None] + update, inside + carried_part)
    cumulative = jnp.cumsum(split_blocks(log_gate), axis=2)
    start_state = jnp.zeros((head_count, key_dim, value_dim), jnp.float32)
    _, outputs = lax.scan(advance, start_state, (split_blocks(query), split_blocks(key_rows), split_blocks(value_rows), cumulative))
    return outputs.transpose(0, 2, 1, 3).reshape(length, head_count, value_dim)

def reference(stream, gate_weight, up_weight, down_weight, query_weight, key_weight, value_weight, outgate_weight, decay_down, decay_up, decay_bias, head_gain, out_weight, norm_gain):

    def ffn_half(current, norm_scale):
        gate = jnp.dot(current, gate_weight, preferred_element_type=jnp.float32)
        upward = jnp.dot(current, up_weight, preferred_element_type=jnp.float32)
        hidden = (jax.nn.silu(gate) * upward).astype(jnp.bfloat16)
        summed = jnp.dot(hidden, down_weight, preferred_element_type=jnp.float32)
        return layer_norm(RESIDUAL_SCALE * current.astype(jnp.float32) + BRANCH_SCALE * summed, norm_scale)

    def one_sequence(sequence):
        first = ffn_half(sequence, norm_gain[0])
        query = jnp.dot(first, query_weight, preferred_element_type=jnp.float32).astype(jnp.bfloat16)
        key_rows = jnp.dot(first, key_weight, preferred_element_type=jnp.float32).astype(jnp.bfloat16)
        value_rows = jnp.dot(first, value_weight, preferred_element_type=jnp.float32).astype(jnp.bfloat16)
        outgate = jnp.dot(first, outgate_weight, preferred_element_type=jnp.float32).astype(jnp.bfloat16)
        low_rank = jnp.dot(first, decay_down, preferred_element_type=jnp.float32).astype(jnp.bfloat16)
        pre_gate = jnp.dot(low_rank, decay_up, preferred_element_type=jnp.float32) + decay_bias
        log_gate = jax.nn.log_sigmoid(pre_gate) / GATE_DIVISOR
        length = first.shape[0]
        mixed = blocked_mixer(query.astype(jnp.float32).reshape(length, HEADS, DK) * DK ** (-0.5), key_rows.astype(jnp.float32).reshape(length, HEADS, DK), value_rows.astype(jnp.float32).reshape(length, HEADS, DV), log_gate.reshape(length, HEADS, DK))
        normed = mixed * lax.rsqrt(lax.optimization_barrier(jnp.mean(mixed * mixed, -1, keepdims=True)) + HEAD_EPS) * head_gain
        gated = (normed.reshape(length, HEADS * DV) * jax.nn.silu(outgate.astype(jnp.float32))).astype(jnp.bfloat16)
        summed = jnp.dot(gated, out_weight, preferred_element_type=jnp.float32)
        second = layer_norm(RESIDUAL_SCALE * first.astype(jnp.float32) + summed, norm_gain[1])
        return ffn_half(second, norm_gain[2])
    sequences = stream.reshape(SEQS, SEQLEN, D)
    return lax.map(one_sequence, sequences).reshape(TOKENS, D)
```

```python
import jax
import jax.numpy as jnp
from jax import lax
from jax.experimental import pallas as pl
from jax.experimental.pallas import tpu as pltpu
from jax.sharding import Mesh, PartitionSpec as P


DK = 64
DV = 128
ROWS = 256
D = 2048
HID = 352
LANE = 128
HEADS = 4
CUTS = (0, 176, 352, 512)
QKVG = 384
LEVELS = 8

RESIDUAL_SCALE = 2.0**0.5
BRANCH_SCALE = 0.5
NORM_EPS = 1e-05
HEAD_EPS = 0.01
GATE_DIVISOR = 16.0

F32 = jnp.float32
BF16 = jnp.bfloat16
ORDERS = ("zxy", "yzx", "xyz")
SIZES = {"x": 4, "y": 4, "c": 2}
VMEM_LIMIT = 60 * 1024 * 1024


def shifted(value, axis, step):
    names, size = (("r", "z"), 8) if axis == "z" else (axis, SIZES[axis])
    return lax.ppermute(value, names, [(i, (i - step) % size) for i in range(size)])


def gathered_direct(value, axis):
    return jnp.stack([value, *(shifted(value, axis, k) for k in (1, 2, -1))])


def gathered_ring(value, axis):
    half = value.shape[0] // 2
    ahead, behind = shifted(value, axis, 1), shifted(value, axis, -1)
    low = shifted(ahead[:half], axis, 1)
    high = shifted(behind[half:], axis, -1)
    return [value, ahead, low, high, behind]


def gathered_pieces(value, order):
    for axis in order[:2]:
        value = gathered_direct(value, axis)
    return gathered_ring(value, order[2])


def block_ref(pieces, order, place):
    first, second, last = order
    at = place[last]
    outer, inner = place[second], place[first]
    if at == 2:
        piece = pieces[2 + outer // 2]
        outer = outer % 2
    else:
        piece = pieces[{0: 0, 1: 1, 3: 4}[at]]
    return piece.at[outer, inner]


def fs_block(place_ref, dz, dx):
    return ((place_ref[0] + dz) % 4) * 4 + (place_ref[1] + dx) % 4


def start_block(src, dst, sem):
    pltpu.make_async_copy(src, dst, sem).start()


def wait_for(ref, sem):
    pltpu.make_async_copy(ref, ref, sem).wait()


def normed(values, gain):
    average = jnp.mean(values, -1, keepdims=True)
    centred = values - average
    spread = jnp.mean(centred * centred, -1, keepdims=True)
    return (centred * lax.rsqrt(spread + NORM_EPS) * gain).astype(BF16)


def after_branch(base_ref, mine_ref, other_ref, gain_ref, scale):
    branch = mine_ref[...].astype(F32) + other_ref[...].astype(F32)
    return normed(RESIDUAL_SCALE * base_ref[...].astype(F32) + scale * branch, gain_ref[...])


def dot_t(a, b):
    return lax.dot_general(a, b, (((1,), (1,)), ((), ())), preferred_element_type=F32)


def ffn_body(place_ref, x, gate_p, up_p, down_p, out_ref, gates, ups, downs, hidden, sem_g, sem_u, sem_d, first_value):
    for y in range(4):
        for pieces, order, dst, sem in ((gate_p, ORDERS[0], gates, sem_g), (up_p, ORDERS[1], ups, sem_u)):
            for dz in range(4):
                for dx in range(4):
                    column = pl.multiple_of(fs_block(place_ref, dz, dx) * LANE, LANE)
                    src = block_ref(pieces, order, {"x": dx, "y": y, "z": dz})
                    start_block(src, dst.at[pl.ds(y * HID, HID), pl.ds(column, LANE)], sem.at[y])
    for dz in range(4):
        for y in range(4):
            for dx in range(4):
                column = pl.multiple_of(fs_block(place_ref, 0, dx) % 4 * LANE, LANE)
                src = block_ref(down_p, ORDERS[2], {"x": dx, "y": y, "z": dz})
                start_block(src, downs.at[dz, pl.ds(y * HID, HID), pl.ds(column, LANE)], sem_d.at[dz])
    x = first_value()
    for pair in range(2):
        rows = pl.ds(2 * pair * HID, 2 * HID)
        for y in (2 * pair, 2 * pair + 1):
            wait_for(gates.at[pl.ds(y * HID, HID)], sem_g.at[y])
            wait_for(ups.at[pl.ds(y * HID, HID)], sem_u.at[y])
        gate = dot_t(x, gates[rows, :])
        upward = dot_t(x, ups[rows, :])
        value = (gate / (1.0 + jnp.exp(-gate)) * upward).astype(BF16)
        hidden[2 * pair] = value[:, :HID]
        hidden[2 * pair + 1] = value[:, HID:]
    units = jnp.concatenate([hidden[y] for y in range(4)], axis=1)
    for dz in range(4):
        wait_for(downs.at[dz], sem_d.at[dz])
        column = pl.multiple_of((place_ref[0] + dz) % 4 * 512, 512)
        part = jnp.dot(units, downs[dz], preferred_element_type=F32)
        out_ref[:, pl.ds(column, 512)] = part.astype(BF16)


def ffn_first_kernel(place_ref, x_ref, *refs):
    gate_p, up_p, down_p = refs[0:5], refs[5:10], refs[10:15]
    out_ref, *scratch = refs[15:]
    ffn_body(place_ref, None, gate_p, up_p, down_p, out_ref, *scratch, lambda: x_ref[...])


def ffn_second_kernel(place_ref, base_ref, mine_ref, other_ref, gain_ref, *refs):
    gate_p, up_p, down_p = refs[0:5], refs[5:10], refs[10:15]
    second_ref, out_ref, *scratch = refs[15:]

    def make():
        second_ref[...] = after_branch(base_ref, mine_ref, other_ref, gain_ref, 1.0)
        return second_ref[...]

    ffn_body(place_ref, None, gate_p, up_p, down_p, out_ref, *scratch, make)


FFN_SCRATCH = (
    pltpu.VMEM((4 * HID, D), BF16),
    pltpu.VMEM((4 * HID, D), BF16),
    pltpu.VMEM((4, 4 * HID, 512), BF16),
    pltpu.VMEM((4, ROWS, HID), BF16),
    pltpu.SemaphoreType.DMA((4,)),
    pltpu.SemaphoreType.DMA((4,)),
    pltpu.SemaphoreType.DMA((4,)),
)


def project_kernel(
    place_ref, base_ref, mine_ref, other_ref, gain_ref, down_ref, up_ref, bias_ref, low_ref, high_ref, *refs
):
    pieces = (refs[0:5], refs[5:10], refs[10:15])
    first_ref, q_ref, k_ref, v_ref, outgate_ref, ghi_ref, glo_ref, state_ref, weights, sem = refs[15:]
    for y in range(4):
        for color in range(3):
            start, stop = CUTS[color], min(CUTS[color + 1], QKVG)
            for dz in range(4):
                for dx in range(4):
                    column = pl.multiple_of(fs_block(place_ref, dz, dx) * LANE, LANE)
                    src = block_ref(pieces[color], ORDERS[color], {"x": dx, "y": y, "z": dz})
                    start_block(
                        src.at[pl.ds(0, stop - start)],
                        weights.at[pl.ds(y * QKVG + start, stop - start), pl.ds(column, LANE)],
                        sem.at[y],
                    )
    first_ref[...] = after_branch(base_ref, mine_ref, other_ref, gain_ref, BRANCH_SCALE)
    first = first_ref[...]
    low = jnp.dot(first, down_ref[...], preferred_element_type=F32).astype(BF16)
    pre = jnp.dot(low, up_ref[...], preferred_element_type=F32) + bias_ref[...]
    log_gate = (jnp.minimum(pre, 0.0) - jnp.log1p(jnp.exp(-jnp.abs(pre)))) / GATE_DIVISOR
    ghi = log_gate.astype(BF16)
    glo = (log_gate - ghi.astype(F32)).astype(BF16)
    ghi_ref[...] = ghi
    glo_ref[...] = glo
    queries, keys = [], []
    for pair in range(2):
        for y in (2 * pair, 2 * pair + 1):
            wait_for(weights.at[pl.ds(y * QKVG, QKVG)], sem.at[y])
        both = dot_t(first, weights[pl.ds(2 * pair * QKVG, 2 * QKVG), :]).astype(BF16)
        a, b = both[:, :QKVG], both[:, QKVG:]
        queries += [a[:, :DK], b[:, :DK]]
        keys += [a[:, DK : 2 * DK], b[:, DK : 2 * DK]]
        for k, part in enumerate((a, b)):
            columns = pl.ds((2 * pair + k) * DV, DV)
            v_ref[:, columns] = part[:, 2 * DK : 2 * DK + DV]
            outgate_ref[:, columns] = part[:, 2 * DK + DV :]
    q_ref[...] = jnp.concatenate(queries, axis=1)
    k_ref[...] = jnp.concatenate(keys, axis=1)
    k32 = k_ref[...].astype(F32)
    since = jnp.dot(low_ref[...], ghi, preferred_element_type=F32) + jnp.dot(
        low_ref[...], glo, preferred_element_type=F32
    )
    until = jnp.dot(high_ref[...], ghi, preferred_element_type=F32) + jnp.dot(
        high_ref[...], glo, preferred_element_type=F32
    )
    kept = k32 * jnp.exp(until)
    q_ref[...] = q_ref[...] * jnp.asarray(DK**-0.5, BF16)
    head = lax.broadcasted_iota(jnp.int32, (ROWS, HEADS * DK), 1) // DK
    state = jnp.zeros((DV, HEADS * DK), F32)
    for h in range(HEADS):
        state += lax.dot_general(
            v_ref[:, h * DV : (h + 1) * DV],
            jnp.where(head == h, kept, 0.0).astype(BF16),
            (((0,), (0,)), ((), ())),
            preferred_element_type=F32,
        )
    state_ref[:DV, :] = state
    state_ref[DV:, :] = jnp.broadcast_to(since[ROWS - 1 :, :], (8, HEADS * DK))


def inside_kernel(q_ref, k_ref, v_ref, ghi_ref, glo_ref, sums_ref, level_ref, mixed_ref, scores):
    q32 = q_ref[...].astype(F32)
    k32 = k_ref[...].astype(F32)
    head = lax.broadcasted_iota(jnp.int32, (ROWS, HEADS * DK), 1) // DK
    level = level_ref[...]

    def products(scale):
        qs = q32 if scale is None else q32 * scale
        ks = k32 if scale is None else k32 * scale
        stacked = jnp.concatenate([jnp.where(head == h, qs, 0.0).astype(BF16) for h in range(HEADS)], axis=0)
        return dot_t(stacked, ks.astype(BF16))

    same = products(None)
    for h in range(HEADS):
        rows = pl.ds(h * ROWS, ROWS)
        scores[rows, :] = jnp.where(level == -1, same[h * ROWS : (h + 1) * ROWS], 0.0)
    for n in range(LEVELS):
        sums = sums_ref[n]
        gap = jnp.dot(sums, ghi_ref[...], preferred_element_type=F32) + jnp.dot(
            sums, glo_ref[...], preferred_element_type=F32
        )
        part = products(jnp.exp(gap))
        for h in range(HEADS):
            rows = pl.ds(h * ROWS, ROWS)
            scores[rows, :] = jnp.where(level == n, part[h * ROWS : (h + 1) * ROWS], scores[rows, :])
    for h in range(HEADS):
        columns = pl.ds(h * DV, DV)
        mixed_ref[:, columns] = jnp.dot(
            scores[pl.ds(h * ROWS, ROWS), :].astype(BF16), v_ref[:, columns], preferred_element_type=F32
        )


def output_kernel(
    place_ref, mixed_ref, q_ref, ghi_ref, glo_ref, outgate_ref, low_ref, gain_ref, s1_ref, s2_ref, s3_ref, *refs
):
    pieces = refs[0:5]
    out_ref, weights, sem = refs[5:]
    skip = QKVG - CUTS[2]
    for y in range(4):
        for dz in range(4):
            for dx in range(4):
                column = pl.multiple_of(fs_block(place_ref, dz, dx) * LANE, LANE)
                src = block_ref(pieces, ORDERS[2], {"x": dx, "y": y, "z": dz})
                start_block(
                    src.at[pl.ds(skip, DV)], weights.at[pl.ds(y * DV, DV), pl.ds(column, LANE)], sem.at[0]
                )
    states = [
        pltpu.roll(ref[...], (HEADS - back) * DK, axis=1) for back, ref in ((1, s1_ref), (2, s2_ref), (3, s3_ref))
    ]
    decay = [s[DV : DV + 1, :] for s in states]
    entering = (
        states[0][:DV]
        + jnp.exp(decay[0]) * states[1][:DV]
        + jnp.exp(decay[0] + decay[1]) * states[2][:DV]
    ).astype(BF16)
    since = jnp.dot(low_ref[...], ghi_ref[...], preferred_element_type=F32) + jnp.dot(
        low_ref[...], glo_ref[...], preferred_element_type=F32
    )
    scaled = q_ref[...].astype(F32) * jnp.exp(since)
    head = lax.broadcasted_iota(jnp.int32, (ROWS, HEADS * DK), 1) // DK
    gated = []
    for h in range(HEADS):
        columns = pl.ds(h * DV, DV)
        mixed = mixed_ref[:, columns] + dot_t(jnp.where(head == h, scaled, 0.0).astype(BF16), entering)
        size = jnp.mean(mixed * mixed, -1, keepdims=True)
        opened = outgate_ref[:, columns].astype(F32)
        opened = opened / (1.0 + jnp.exp(-opened))
        gated.append((mixed * lax.rsqrt(size + HEAD_EPS) * gain_ref[...] * opened).astype(BF16))
    channels = jnp.concatenate(gated, axis=1)
    wait_for(weights, sem.at[0])
    for n in range(4):
        columns = pl.ds(n * 512, 512)
        out_ref[:, columns] = jnp.dot(channels, weights[:, columns], preferred_element_type=F32).astype(BF16)


def call(kernel, outs, scalars, arrays, pieces, scratch, flops):
    in_specs = (
        [pl.BlockSpec(memory_space=pltpu.SMEM)] * len(scalars)
        + [pl.BlockSpec(memory_space=pltpu.VMEM)] * len(arrays)
        + [pl.BlockSpec(memory_space=pltpu.HBM)] * len(pieces)
    )
    return pl.pallas_call(
        kernel,
        out_shape=[jax.ShapeDtypeStruct(*out) for out in outs],
        in_specs=in_specs,
        out_specs=[pl.BlockSpec(memory_space=pltpu.VMEM)] * len(outs),
        scratch_shapes=scratch,
        compiler_params=pltpu.CompilerParams(vmem_limit_bytes=VMEM_LIMIT),
        cost_estimate=pl.CostEstimate(flops=flops, bytes_accessed=20_000_000, transcendentals=0),
    )(*scalars, *arrays, *pieces)


def decay_sums():
    t = jnp.arange(ROWS)[:, None]
    s = jnp.arange(ROWS)[None, :]
    low, high = s <= t, s > t
    levels = []
    level = jnp.where(s == t, -1, LEVELS)
    for n in range(LEVELS):
        same = (t >> n) == (s >> n)
        levels.append(same & jnp.where((t >> n) & 1 == 1, low, high))
        level = jnp.where((s < t) & ((t >> n) != (s >> n)), n, level)
    return low.astype(BF16), high.astype(BF16), jnp.stack(levels).astype(BF16), level.astype(jnp.int32)


def on_device(
    stream,
    gate_weight,
    up_weight,
    down_weight,
    query_weight,
    key_weight,
    value_weight,
    outgate_weight,
    decay_down,
    decay_up,
    decay_bias,
    head_gain,
    out_weight,
    norm_gain,
):
    core = lax.axis_index("c")
    place = jnp.stack([lax.axis_index("z"), lax.axis_index("x")]).astype(jnp.int32)

    def swapped(value):
        return lax.ppermute(value, "c", [(0, 1), (1, 0)])

    def own_rows(value):
        return lax.dynamic_slice_in_dim(value, core * 128, 128, 0)

    other = swapped(stream)
    rows = jnp.where(core == 0, jnp.concatenate([stream, other]), jnp.concatenate([other, stream]))

    ffn_pieces = [
        gathered_pieces(shard, order) for shard, order in zip((gate_weight.T, up_weight.T, down_weight), ORDERS)
    ]
    attention = jnp.concatenate([query_weight, key_weight, value_weight, outgate_weight], axis=1).T
    attention = jnp.concatenate([attention, out_weight], axis=0)
    mix_pieces = [
        gathered_pieces(attention[CUTS[n] : CUTS[n + 1]], order) for n, order in enumerate(ORDERS)
    ]
    decay = jnp.concatenate(
        [decay_up.astype(F32), decay_bias[None, :], jnp.zeros((7, DK), F32)], axis=0
    )
    decay = jnp.concatenate([decay, *(shifted(decay, "y", k) for k in (1, 2, 3))], axis=1)
    low, high, sums, level = decay_sums()

    flat_ffn = [p for pieces in ffn_pieces for p in pieces]
    flat_mix = [p for pieces in mix_pieces for p in pieces]

    (part,) = call(
        ffn_first_kernel, [((ROWS, D), BF16)], [place], [rows], flat_ffn, FFN_SCRATCH, 4_400_000_000
    )
    wide = ((ROWS, HEADS * DK), BF16)
    broad = ((ROWS, HEADS * DV), BF16)
    first, query, keys, values, outgate, ghi, glo, state = call(
        project_kernel,
        [((ROWS, D), BF16), wide, wide, broad, broad, wide, wide, ((DV + 8, HEADS * DK), F32)],
        [place],
        [
            rows,
            part,
            swapped(part),
            norm_gain[0:1],
            decay_down,
            decay[:32].astype(BF16),
            decay[32:33],
            low,
            high,
        ],
        flat_mix,
        [pltpu.VMEM((4 * QKVG, D), BF16), pltpu.SemaphoreType.DMA((4,))],
        2_000_000_000,
    )
    earlier = [
        lax.ppermute(state, "y", [(i, i + back) for i in range(4 - back)]) for back in (1, 2, 3)
    ]
    (mixed,) = call(
        inside_kernel,
        [((ROWS, HEADS * DV), F32)],
        [],
        [query, keys, values, ghi, glo, sums, level],
        [],
        [pltpu.VMEM((HEADS * ROWS, ROWS), F32)],
        4_000_000_000,
    )
    (part,) = call(
        output_kernel,
        [((ROWS, D), BF16)],
        [place],
        [mixed, query, ghi, glo, outgate, low, head_gain[None, :], *earlier],
        mix_pieces[2],
        [pltpu.VMEM((4 * DV, D), BF16), pltpu.SemaphoreType.DMA((1,))],
        1_000_000_000,
    )
    second, part = call(
        ffn_second_kernel,
        [((ROWS, D), BF16), ((ROWS, D), BF16)],
        [place],
        [first, part, swapped(part), norm_gain[1:2]],
        flat_ffn,
        FFN_SCRATCH,
        4_400_000_000,
    )
    theirs = swapped(lax.dynamic_slice_in_dim(part, (1 - core) * 128, 128, 0))
    branch = own_rows(part).astype(F32) + theirs.astype(F32)
    return normed(RESIDUAL_SCALE * own_rows(second).astype(F32) + BRANCH_SCALE * branch, norm_gain[2:3])


def solution(mesh):
    fine = Mesh(mesh.devices.reshape(2, 4, 4, 4, 2), ("r", "z", "x", "y", "c"))
    fs, tp = ("z", "x"), ("y", "c")
    in_specs = (
        P(("r", *fs, *tp), None),
        P(fs, tp),
        P(fs, tp),
        P(tp, fs),
        P(fs, tp),
        P(fs, tp),
        P(fs, tp),
        P(fs, tp),
        P(),
        P(None, tp),
        P(tp),
        P(),
        P(tp, fs),
        P(),
    )
    return jax.shard_map(
        on_device, mesh=fine, in_specs=in_specs, out_specs=P(("r", *fs, *tp), None), check_vma=False
    )
```

```python
import jax
import jax.numpy as jnp
import numpy as np
from jax import lax
from jax.experimental import pallas as pl
from jax.experimental.pallas import tpu as pltpu
from jax.sharding import Mesh, PartitionSpec as P


DK = 64
DV = 128
ROWS = 256
D = 2048
HID = 352
LANE = 128
HEADS = 4
MIX = 352
TAIL = 32
LEVELS = 8

RESIDUAL_SCALE = 2.0**0.5
BRANCH_SCALE = 0.5
NORM_EPS = 1e-05
HEAD_EPS = 0.01
GATE_DIVISOR = 16.0

F32 = jnp.float32
BF16 = jnp.bfloat16
LARGE = ("zxy", "yzx")
SMALL = ("xyz", "xyz")
AXES = {"r": 2, "z": 4, "x": 4, "y": 4, "c": 2}
VMEM_LIMIT = 20 * 1024 * 1024


def shifted(value, axes, step):
    pairs = []
    for n in range(256):
        r, z, x, y, c = (int(i) for i in np.unravel_index(n, tuple(AXES.values())))
        axis = axes[c]
        if axis == "z":
            ring = 4 * r + z
            go = -step if step == 2 and ring % 2 else step
            r, z = divmod((ring - go) % 8, 4)
        elif axis == "x":
            x = (x - step) % 4
        else:
            y = (y - step) % 4
        pairs.append((n, int(np.ravel_multi_index((r, z, x, y, c), tuple(AXES.values())))))
    return lax.ppermute(value, tuple(AXES), pairs)


def gathered_direct(value, axis):
    return [value, *(shifted(value, axis, k) for k in (1, 2, -1))]


def gathered_ring(halves, axis):
    low, high = halves
    behind_high = shifted(high, axis, -1)
    ahead_low = shifted(low, axis, 1)
    behind_low = shifted(low, axis, -1)
    ahead_high = shifted(high, axis, 1)
    far_low = shifted(ahead_low, axis, 1)
    far_high = shifted(behind_high, axis, -1)
    return [low, high, ahead_low, ahead_high, far_low, far_high, behind_low, behind_high]


def gathered_planes(value, orders):
    first, second, _ = zip(*orders)
    line = gathered_direct(value, first)
    line = call(stack_kernel, [((4, *value.shape), BF16)], [], line)[0]
    return gathered_direct(line, second)


def last_of(orders):
    return tuple(order[2] for order in orders)


def fs_block(place_ref, dz, dx):
    return ((place_ref[0] + dz) % 4) * 4 + (place_ref[1] + dx) % 4


def normed(values, gain):
    average = jnp.mean(values, -1, keepdims=True)
    centred = values - average
    spread = jnp.mean(centred * centred, -1, keepdims=True)
    return (centred * lax.rsqrt(spread + NORM_EPS) * gain).astype(BF16)


def after_branch(base_ref, mine_ref, other_ref, gain_ref, scale):
    branch = mine_ref[...].astype(F32) + other_ref[...].astype(F32)
    return normed(RESIDUAL_SCALE * base_ref[...].astype(F32) + scale * branch, gain_ref[...])


def dot_t(a, b):
    return lax.dot_general(a, b, (((1,), (1,)), ((), ())), preferred_element_type=F32)


def ordered_columns(place_ref, ref):
    blocks = []
    for dx in range(4):
        for dz in range(4):
            blocks.append(ref[:, pl.ds(pl.multiple_of(fs_block(place_ref, dz, dx) * LANE, LANE), LANE)])
    return jnp.concatenate(blocks, axis=1)


def joined_features(block):
    return jnp.concatenate([block(dx, dz) for dx in range(4) for dz in range(4)], axis=1)


def prepare_kernel(gate_ref, up_ref, query_ref, key_ref, value_ref, outgate_ref, down_ref, out_ref, large, small):
    row = 0
    for ref in (gate_ref, up_ref, query_ref, key_ref):
        large[row : row + ref.shape[0], :] = ref[...]
        row += ref.shape[0]
    large[row : row + DV, :] = value_ref[...].astype(F32).T.astype(BF16)
    row += DV
    outgate = outgate_ref[...].astype(F32).T.astype(BF16)
    large[row:, :] = outgate[: DV - TAIL]
    small[:HID, :] = down_ref[...]
    small[HID : HID + TAIL, :] = outgate[DV - TAIL :]
    small[HID + TAIL :, :] = out_ref[...]


def stack_kernel(*refs):
    for n in range(4):
        refs[4][n] = refs[n][...]


def divide_kernel(*refs):
    planes, (low, high, mix) = refs[:4], refs[4:]
    units = low.shape[2]
    for n, plane in enumerate(planes):
        (low, high)[n // 2][n % 2] = plane[:, :units]
        mix[n] = plane[:, units:]


def ffn_body(place_ref, large_p, small_p, out_ref, hidden, first_ref):
    x = ordered_columns(place_ref, first_ref())

    def units_of(y, block):
        both = dot_t(x, joined_features(block))
        gate, upward = both[:, :HID], both[:, HID:]
        hidden[y] = (gate / (1.0 + jnp.exp(-gate)) * upward).astype(BF16)

    @pl.when(place_ref[2] == 0)
    def _():
        for y in range(4):
            units_of(y, lambda dx, dz: large_p[2 * y + dx // 2][dx % 2, dz])

    @pl.when(place_ref[2] == 1)
    def _():
        @pl.loop(0, 4)
        def _(y):
            units_of(y, lambda dx, dz: large_p[2 * dx + dz // 2][dz % 2, y])

    units = jnp.concatenate([hidden[y] for y in range(4)], axis=1)
    for dz in range(4):
        columns = [
            jnp.concatenate([small_p[2 * dz + y // 2][y % 2, dx] for y in range(4)], axis=0) for dx in range(4)
        ]
        part = jnp.dot(units, jnp.concatenate(columns, axis=1), preferred_element_type=F32).astype(BF16)
        for dx in range(4):
            column = pl.multiple_of(fs_block(place_ref, dz, dx) * LANE, LANE)
            out_ref[:, pl.ds(column, LANE)] = part[:, dx * LANE : (dx + 1) * LANE]


def ffn_first_kernel(place_ref, x_ref, *refs):
    out_ref, *scratch = refs[16:]
    ffn_body(place_ref, refs[0:8], refs[8:16], out_ref, *scratch, lambda: x_ref)


def ffn_second_kernel(place_ref, base_ref, mine_ref, other_ref, gain_ref, *refs):
    second_ref, out_ref, *scratch = refs[16:]

    def make():
        second_ref[...] = after_branch(base_ref, mine_ref, other_ref, gain_ref, 1.0)
        return second_ref

    ffn_body(place_ref, refs[0:8], refs[8:16], out_ref, *scratch, make)


FFN_SCRATCH = (pltpu.VMEM((4, ROWS, HID), BF16),)


def position_masks():
    t = lax.broadcasted_iota(jnp.int32, (ROWS, ROWS), 0)
    s = lax.broadcasted_iota(jnp.int32, (ROWS, ROWS), 1)
    return t, s


def summed(mask, high, low):
    ones = jnp.where(mask, 1.0, 0.0).astype(BF16)
    return jnp.dot(ones, high, preferred_element_type=F32) + jnp.dot(ones, low, preferred_element_type=F32)


def project_kernel(place_ref, base_ref, mine_ref, other_ref, gain_ref, down_ref, up_ref, bias_ref, *refs):
    first_ref, q_ref, k_ref, v_ref, outgate_ref, ghi_ref, glo_ref, state_ref, parts = refs[8:]
    large_p, small_p = refs[:4], refs[4:8]
    first_ref[...] = after_branch(base_ref, mine_ref, other_ref, gain_ref, BRANCH_SCALE)
    first = first_ref[...]
    low = jnp.dot(first, down_ref[...], preferred_element_type=F32).astype(BF16)
    pre = jnp.dot(low, up_ref[...], preferred_element_type=F32) + bias_ref[...]
    log_gate = (jnp.minimum(pre, 0.0) - jnp.log1p(jnp.exp(-jnp.abs(pre)))) / GATE_DIVISOR
    ghi = log_gate.astype(BF16)
    glo = (log_gate - ghi.astype(F32)).astype(BF16)
    ghi_ref[...] = ghi
    glo_ref[...] = glo
    x = ordered_columns(place_ref, first_ref)

    def part_of(y, block, tail):
        rows = jnp.concatenate([joined_features(block), joined_features(tail)], axis=0)
        parts[y] = dot_t(x, rows).astype(BF16)

    @pl.when(place_ref[2] == 0)
    def _():
        for y in range(4):
            part_of(y, lambda dx, dz: large_p[y][dx, dz], lambda dx, dz: small_p[dz][y, dx, :TAIL])

    @pl.when(place_ref[2] == 1)
    def _():
        @pl.loop(0, 4)
        def _(y):
            part_of(y, lambda dx, dz: large_p[dx][dz, y], lambda dx, dz: small_p[dz][y, dx, :TAIL])

    queries, keys = [], []
    for y in range(4):
        queries.append(parts[y, :, :DK])
        keys.append(parts[y, :, DK : 2 * DK])
        v_ref[:, pl.ds(y * DV, DV)] = parts[y, :, 2 * DK : 2 * DK + DV]
        outgate_ref[:, pl.ds(y * DV, DV)] = parts[y, :, 2 * DK + DV :]
    q_ref[...] = jnp.concatenate(queries, axis=1)
    k_ref[...] = jnp.concatenate(keys, axis=1)
    k32 = k_ref[...].astype(F32)
    t, s = position_masks()
    since = summed(s <= t, ghi, glo)
    until = summed(s > t, ghi, glo)
    kept = k32 * jnp.exp(until)
    q_ref[...] = q_ref[...] * jnp.asarray(DK**-0.5, BF16)
    head = lax.broadcasted_iota(jnp.int32, (ROWS, HEADS * DK), 1) // DK
    state = jnp.zeros((DV, HEADS * DK), F32)
    for h in range(HEADS):
        state += lax.dot_general(
            v_ref[:, h * DV : (h + 1) * DV],
            jnp.where(head == h, kept, 0.0).astype(BF16),
            (((0,), (0,)), ((), ())),
            preferred_element_type=F32,
        )
    state_ref[:DV, :] = state
    state_ref[DV:, :] = jnp.broadcast_to(since[ROWS - 1 :, :], (8, HEADS * DK))


def inside_kernel(q_ref, k_ref, v_ref, ghi_ref, glo_ref, mixed_ref, scores):
    q32 = q_ref[...].astype(F32)
    k32 = k_ref[...].astype(F32)
    head = lax.broadcasted_iota(jnp.int32, (ROWS, HEADS * DK), 1) // DK
    t, s = position_masks()

    def products(qs, ks):
        stacked = jnp.concatenate([jnp.where(head == h, qs, 0.0).astype(BF16) for h in range(HEADS)], axis=0)
        return dot_t(stacked, ks.astype(BF16))

    same = products(q32, k32)
    for h in range(HEADS):
        rows = pl.ds(h * ROWS, ROWS)
        scores[rows, :] = jnp.where(t == s, same[h * ROWS : (h + 1) * ROWS], 0.0)

    @pl.loop(0, LEVELS)
    def _(n):
        tn, sn = t >> n, s >> n
        upper = (tn & 1) == 1
        gap = summed((tn == sn) & ((upper & (s <= t)) | (~upper & (s > t))), ghi_ref[...], glo_ref[...])
        scale = jnp.exp(gap)
        part = products(q32 * scale, k32 * scale)
        chosen = upper & (tn == sn + 1)
        for h in range(HEADS):
            rows = pl.ds(h * ROWS, ROWS)
            scores[rows, :] = jnp.where(chosen, part[h * ROWS : (h + 1) * ROWS], scores[rows, :])

    for h in range(HEADS):
        columns = pl.ds(h * DV, DV)
        mixed_ref[:, columns] = jnp.dot(
            scores[pl.ds(h * ROWS, ROWS), :].astype(BF16), v_ref[:, columns], preferred_element_type=F32
        )


def output_kernel(
    place_ref, mixed_ref, q_ref, ghi_ref, glo_ref, outgate_ref, gain_ref, s1_ref, s2_ref, s3_ref, *refs
):
    (out_ref,) = refs[4:]
    states = [
        pltpu.roll(ref[...], (HEADS - back) * DK, axis=1) for back, ref in ((1, s1_ref), (2, s2_ref), (3, s3_ref))
    ]
    decay = [s[DV : DV + 1, :] for s in states]
    entering = (
        states[0][:DV]
        + jnp.exp(decay[0]) * states[1][:DV]
        + jnp.exp(decay[0] + decay[1]) * states[2][:DV]
    ).astype(BF16)
    t, s = position_masks()
    since = summed(s <= t, ghi_ref[...], glo_ref[...])
    scaled = q_ref[...].astype(F32) * jnp.exp(since)
    head = lax.broadcasted_iota(jnp.int32, (ROWS, HEADS * DK), 1) // DK
    gated = []
    for h in range(HEADS):
        columns = pl.ds(h * DV, DV)
        mixed = mixed_ref[:, columns] + dot_t(jnp.where(head == h, scaled, 0.0).astype(BF16), entering)
        size = jnp.mean(mixed * mixed, -1, keepdims=True)
        opened = outgate_ref[:, columns].astype(F32)
        opened = opened / (1.0 + jnp.exp(-opened))
        gated.append((mixed * lax.rsqrt(size + HEAD_EPS) * gain_ref[...] * opened).astype(BF16))
    channels = jnp.concatenate(gated, axis=1)
    for dz in range(4):
        columns = [jnp.concatenate([refs[dz][y, dx, TAIL:] for y in range(4)], axis=0) for dx in range(4)]
        part = jnp.dot(channels, jnp.concatenate(columns, axis=1), preferred_element_type=F32).astype(BF16)
        for dx in range(4):
            column = pl.multiple_of(fs_block(place_ref, dz, dx) * LANE, LANE)
            out_ref[:, pl.ds(column, LANE)] = part[:, dx * LANE : (dx + 1) * LANE]


def call(kernel, outs, scalars, arrays, scratch=(), flops=1_000_000):
    in_specs = [pl.BlockSpec(memory_space=pltpu.SMEM)] * len(scalars) + [
        pl.BlockSpec(memory_space=pltpu.VMEM)
    ] * len(arrays)
    return pl.pallas_call(
        kernel,
        out_shape=[jax.ShapeDtypeStruct(*out) for out in outs],
        in_specs=in_specs,
        out_specs=[pl.BlockSpec(memory_space=pltpu.VMEM)] * len(outs),
        scratch_shapes=scratch,
        compiler_params=pltpu.CompilerParams(vmem_limit_bytes=VMEM_LIMIT),
        cost_estimate=pl.CostEstimate(flops=flops, bytes_accessed=1_000_000, transcendentals=0),
    )(*scalars, *arrays)


def on_device(
    stream,
    gate_weight,
    up_weight,
    down_weight,
    query_weight,
    key_weight,
    value_weight,
    outgate_weight,
    decay_down,
    decay_up,
    decay_bias,
    head_gain,
    out_weight,
    norm_gain,
):
    core = lax.axis_index("c")
    place = jnp.stack([lax.axis_index("z"), lax.axis_index("x"), core]).astype(jnp.int32)

    def swapped(value):
        return lax.ppermute(value, "c", [(0, 1), (1, 0)])

    def own_rows(value):
        return lax.dynamic_slice_in_dim(value, core * 128, 128, 0)

    other = swapped(stream)
    rows = jnp.where(core == 0, jnp.concatenate([stream, other]), jnp.concatenate([other, stream]))

    large, small = call(
        prepare_kernel,
        [((2 * HID + MIX, LANE), BF16), ((HID + TAIL + DV, LANE), BF16)],
        [],
        [
            gate_weight.T,
            up_weight.T,
            query_weight.T,
            key_weight.T,
            value_weight,
            outgate_weight,
            down_weight,
            out_weight,
        ],
    )
    flat_ffn, flat_mix = [], []
    for shard, orders, units in ((small, SMALL, HID), (large, LARGE, 2 * HID)):
        planes = gathered_planes(shard, orders)
        rest = shard.shape[0] - units
        low, high, mix = call(
            divide_kernel,
            [((2, 4, units, LANE), BF16), ((2, 4, units, LANE), BF16), ((4, 4, rest, LANE), BF16)],
            [],
            planes,
        )
        flat_ffn = gathered_ring((low, high), last_of(orders)) + flat_ffn
        flat_mix = gathered_direct(mix, last_of(orders)) + flat_mix
    decay = jnp.concatenate(
        [decay_up.astype(F32), decay_bias[None, :], jnp.zeros((7, DK), F32)], axis=0
    )
    shifts = [shifted(decay, "yy", k) for k in (1, 2, 3)]
    decay = jnp.concatenate([decay, *shifts], axis=1)

    (part,) = call(
        ffn_first_kernel, [((ROWS, D), BF16)], [place], [rows, *flat_ffn], FFN_SCRATCH, 4_400_000_000
    )
    wide = ((ROWS, HEADS * DK), BF16)
    broad = ((ROWS, HEADS * DV), BF16)
    first, query, keys, values, outgate, ghi, glo, state = call(
        project_kernel,
        [((ROWS, D), BF16), wide, wide, broad, broad, wide, wide, ((DV + 8, HEADS * DK), F32)],
        [place],
        [
            rows,
            part,
            swapped(part),
            norm_gain[0:1],
            decay_down,
            decay[:32].astype(BF16),
            decay[32:33],
            *flat_mix,
        ],
        [pltpu.VMEM((4, ROWS, MIX + TAIL), BF16)],
        2_000_000_000,
    )
    earlier = [
        lax.ppermute(state, "y", [(i, i + back) for i in range(4 - back)]) for back in (1, 2, 3)
    ]
    (mixed,) = call(
        inside_kernel,
        [((ROWS, HEADS * DV), F32)],
        [],
        [query, keys, values, ghi, glo],
        [pltpu.VMEM((HEADS * ROWS, ROWS), F32)],
        4_000_000_000,
    )
    (part,) = call(
        output_kernel,
        [((ROWS, D), BF16)],
        [place],
        [mixed, query, ghi, glo, outgate, head_gain[None, :], *earlier, *flat_mix[4:]],
        (),
        1_000_000_000,
    )
    second, part = call(
        ffn_second_kernel,
        [((ROWS, D), BF16), ((ROWS, D), BF16)],
        [place],
        [first, part, swapped(part), norm_gain[1:2], *flat_ffn],
        FFN_SCRATCH,
        4_400_000_000,
    )
    theirs = swapped(lax.dynamic_slice_in_dim(part, (1 - core) * 128, 128, 0))
    branch = own_rows(part).astype(F32) + theirs.astype(F32)
    return normed(RESIDUAL_SCALE * own_rows(second).astype(F32) + BRANCH_SCALE * branch, norm_gain[2:3])


def solution(mesh):
    fine = Mesh(mesh.devices.reshape(2, 4, 4, 4, 2), ("r", "z", "x", "y", "c"))
    fs, tp = ("z", "x"), ("y", "c")
    in_specs = (
        P(("r", *fs, *tp), None),
        P(fs, tp),
        P(fs, tp),
        P(tp, fs),
        P(fs, tp),
        P(fs, tp),
        P(fs, tp),
        P(fs, tp),
        P(),
        P(None, tp),
        P(tp),
        P(),
        P(tp, fs),
        P(),
    )
    return jax.shard_map(on_device, mesh=fine, in_specs=in_specs, out_specs=P(("r", *fs, *tp), None), check_vma=False)
```

```python
import jax
import jax.numpy as jnp
import numpy as np
from jax import lax
from jax.experimental import pallas as pl
from jax.experimental.pallas import tpu as pltpu
from jax.sharding import Mesh, PartitionSpec as P


DK = 64
DV = 128
ROWS = 256
D = 2048
HID = 352
LANE = 128
HEADS = 4
MIX = 352
TAIL = 32
LEVELS = 8

RESIDUAL_SCALE = 2.0**0.5
BRANCH_SCALE = 0.5
NORM_EPS = 1e-05
HEAD_EPS = 0.01
GATE_DIVISOR = 16.0

F32 = jnp.float32
BF16 = jnp.bfloat16
LARGE = ("zxy", "yzx")
SMALL = ("xyz", "xyz")
AXES = {"r": 2, "z": 4, "x": 4, "y": 4, "c": 2}
VMEM_LIMIT = 20 * 1024 * 1024


def shifted(value, axes, step):
    pairs = []
    for n in range(256):
        r, z, x, y, c = (int(i) for i in np.unravel_index(n, tuple(AXES.values())))
        axis = axes[c]
        if axis == "z":
            ring = 4 * r + z
            go = -step if step == 2 and ring % 2 else step
            r, z = divmod((ring - go) % 8, 4)
        elif axis == "x":
            x = (x - step) % 4
        else:
            y = (y - step) % 4
        pairs.append((n, int(np.ravel_multi_index((r, z, x, y, c), tuple(AXES.values())))))
    return lax.ppermute(value, tuple(AXES), pairs)


def gathered_direct(value, axis):
    ahead, behind = shifted(value, axis, 1), shifted(value, axis, -1)
    return [value, ahead, shifted(value, axis, 2), behind]


def gathered_ring(low, high, axis):
    ahead_low, behind_low = shifted(low, axis, 1), shifted(low, axis, -1)
    behind_high, ahead_high = shifted(high, axis, -1), shifted(high, axis, 1)
    far_low = shifted(ahead_low, axis, 1)
    far_high = shifted(behind_high, axis, -1)
    return [low, high, ahead_low, ahead_high, far_low, far_high, behind_low, behind_high]


def gathered_planes(value, orders):
    first, second, _ = zip(*orders)
    line = gathered_direct(value, first)
    line = call(stack_kernel, [((4, *value.shape), BF16)], [], line)[0]
    return gathered_direct(line, second)


def last_of(orders):
    return tuple(order[2] for order in orders)


def fs_block(place_ref, dz, dx):
    return ((place_ref[0] + dz) % 4) * 4 + (place_ref[1] + dx) % 4


def normed(values, gain):
    average = jnp.mean(values, -1, keepdims=True)
    centred = values - average
    spread = jnp.mean(centred * centred, -1, keepdims=True)
    return (centred * lax.rsqrt(spread + NORM_EPS) * gain).astype(BF16)


def after_branch(out_ref, base_ref, mine_ref, other_ref, gain_ref, scale):
    @pl.loop(0, out_ref.shape[0] // 64)
    def _(n):
        rows = pl.ds(pl.multiple_of(n * 64, 64), 64)
        branch = mine_ref[rows, :].astype(F32) + other_ref[rows, :].astype(F32)
        out_ref[rows, :] = normed(RESIDUAL_SCALE * base_ref[rows, :].astype(F32) + scale * branch, gain_ref[...])


def dot_t(a, b):
    return lax.dot_general(a, b, (((1,), (1,)), ((), ())), preferred_element_type=F32)


def ordered_columns(place_ref, ref):
    blocks = []
    for dx in range(4):
        for dz in range(4):
            blocks.append(ref[:, pl.ds(pl.multiple_of(fs_block(place_ref, dz, dx) * LANE, LANE), LANE)])
    return jnp.concatenate(blocks, axis=1)


def joined_features(block):
    return jnp.concatenate([block(dx, dz) for dx in range(4) for dz in range(4)], axis=1)


def prepare_kernel(gate_ref, up_ref, query_ref, key_ref, value_ref, outgate_ref, down_ref, out_ref, *refs):
    large, small, value, outgate, sem = refs
    row, copies = 0, []
    for ref in (gate_ref, up_ref, query_ref, key_ref):
        copies.append((ref, large.at[pl.ds(row, ref.shape[0])]))
        row += ref.shape[0]
    copies += [(down_ref, small.at[pl.ds(0, HID)]), (out_ref, small.at[pl.ds(HID + TAIL, DV)])]
    copies += [(value_ref, value), (outgate_ref, outgate)]
    copies = [pltpu.make_async_copy(*pair, sem.at[n]) for n, pair in enumerate(copies)]
    for copy in copies:
        copy.start()
    for copy in copies:
        copy.wait()
    large[row : row + DV, :] = value[...].astype(F32).T.astype(BF16)
    turned = outgate[...].astype(F32).T.astype(BF16)
    large[row + DV :, :] = turned[: DV - TAIL]
    small[HID : HID + TAIL, :] = turned[DV - TAIL :]


def stack_kernel(*refs):
    for n in range(4):
        refs[4][n] = refs[n][...]


def divide_low_kernel(plane, ahead, low):
    units = low.shape[2]
    low[0] = plane[:, :units]
    low[1] = ahead[:, :units]


def divide_high_kernel(*refs):
    planes, (high, mix) = refs[:4], refs[4:]
    units = high.shape[2]
    for n, plane in enumerate(planes):
        if n > 1:
            high[n - 2] = plane[:, :units]
        mix[n] = plane[:, units:]


def arranged(place_ref, pieces, halves, y, dst):
    inner = 4 // halves
    for k in range(4):

        @pl.when((place_ref[2] == 0) & (y == k))
        def _():
            for half in range(halves):

                @pl.loop(0, inner)
                def _(n):
                    for dz in range(4):
                        dst[half * inner + n, dz] = pieces[halves * k + half][n, dz]

    @pl.when(place_ref[2] == 1)
    def _():
        for dx in range(4):
            for half in range(halves):

                @pl.loop(0, inner)
                def _(n):
                    dst[dx, half * inner + n] = pieces[halves * dx + half][n, y]


def hidden_units(x, large, y, hidden):
    both = dot_t(x, joined_features(lambda dx, dz: large[y, dx, dz]))
    gate, upward = both[:, :HID], both[:, HID:]
    hidden[y] = (gate / (1.0 + jnp.exp(-gate)) * upward).astype(BF16)


def projected(place_ref, units, block, store):
    @pl.loop(0, 4)
    def _(dx):
        columns = [jnp.concatenate([block(dz, y, dx) for y in range(4)], axis=0) for dz in range(4)]
        part = jnp.dot(units(), jnp.concatenate(columns, axis=1), preferred_element_type=F32).astype(BF16)
        for dz in range(4):
            column = pl.multiple_of(fs_block(place_ref, dz, dx) * LANE, LANE)
            store(pl.ds(column, LANE), part[:, dz * LANE : (dz + 1) * LANE])


def ffn_first_kernel(place_ref, x_ref, *refs):
    large_p, small_p = refs[:8], refs[8:16]
    out_ref, large_ref, hidden = refs[16:]
    x = ordered_columns(place_ref, x_ref)

    @pl.loop(0, 4)
    def _(y):
        arranged(place_ref, large_p, 2, y, large_ref.at[y])
        hidden_units(x, large_ref, y, hidden)

    def store(columns, value):
        out_ref[:, columns] = value

    projected(
        place_ref,
        lambda: jnp.concatenate([hidden[y] for y in range(4)], axis=1),
        lambda dz, y, dx: small_p[2 * dz + y // 2][y % 2, dx],
        store,
    )


def ffn_second_kernel(place_ref, base_ref, mine_ref, other_ref, gain_ref, large_ref, *refs):
    small_p = refs[:8]
    own_ref, keep_ref, give_ref, hidden, second = refs[8:]
    core = place_ref[2]
    after_branch(second, base_ref, mine_ref, other_ref, gain_ref, 1.0)
    own_ref[...] = second[pl.ds(pl.multiple_of(core * 128, 128), 128), :]
    x = ordered_columns(place_ref, second)

    @pl.loop(0, 4)
    def _(y):
        hidden_units(x, large_ref, y, hidden)

    def store(columns, value):
        keep_ref[:, columns] = jnp.where(core == 0, value[:128], value[128:])
        give_ref[:, columns] = jnp.where(core == 0, value[128:], value[:128])

    projected(
        place_ref,
        lambda: jnp.concatenate([hidden[y] for y in range(4)], axis=1),
        lambda dz, y, dx: small_p[2 * dz + y // 2][y % 2, dx],
        store,
    )


def last_norm_kernel(base_ref, mine_ref, other_ref, gain_ref, out_ref):
    after_branch(out_ref, base_ref, mine_ref, other_ref, gain_ref, BRANCH_SCALE)


FFN_SCRATCH = (pltpu.VMEM((4, ROWS, HID), BF16),)


def position_masks():
    t = lax.broadcasted_iota(jnp.int32, (ROWS, ROWS), 0)
    s = lax.broadcasted_iota(jnp.int32, (ROWS, ROWS), 1)
    return t, s


def summed(mask, high, low):
    ones = jnp.where(mask, 1.0, 0.0).astype(BF16)
    return jnp.dot(ones, high, preferred_element_type=F32) + jnp.dot(ones, low, preferred_element_type=F32)


def project_kernel(place_ref, base_ref, mine_ref, other_ref, gain_ref, down_ref, up_ref, bias_ref, *refs):
    first_ref, q_ref, k_ref, v_ref, outgate_ref, ghi_ref, glo_ref, state_ref, parts, large = refs[8:]
    large_p, small_p = refs[:4], refs[4:8]
    after_branch(first_ref, base_ref, mine_ref, other_ref, gain_ref, BRANCH_SCALE)
    first = first_ref[...]
    low = dot_t(first, down_ref[...]).astype(BF16)
    pre = jnp.dot(low, up_ref[...], preferred_element_type=F32) + bias_ref[...]
    log_gate = (jnp.minimum(pre, 0.0) - jnp.log1p(jnp.exp(-jnp.abs(pre)))) / GATE_DIVISOR
    ghi = log_gate.astype(BF16)
    glo = (log_gate - ghi.astype(F32)).astype(BF16)
    ghi_ref[...] = ghi
    glo_ref[...] = glo
    x = ordered_columns(place_ref, first_ref)

    @pl.loop(0, 4)
    def _(y):
        arranged(place_ref, large_p, 1, y, large)
        rows = [
            joined_features(lambda dx, dz: large[dx, dz]),
            joined_features(lambda dx, dz: small_p[dz][y, dx, :TAIL]),
        ]
        parts[y] = dot_t(x, jnp.concatenate(rows, axis=0)).astype(BF16)

    queries, keys = [], []
    for y in range(4):
        queries.append(parts[y, :, :DK])
        keys.append(parts[y, :, DK : 2 * DK])
        v_ref[:, pl.ds(y * DV, DV)] = parts[y, :, 2 * DK : 2 * DK + DV]
        outgate_ref[:, pl.ds(y * DV, DV)] = parts[y, :, 2 * DK + DV :]
    q_ref[...] = jnp.concatenate(queries, axis=1)
    k_ref[...] = jnp.concatenate(keys, axis=1)
    k32 = k_ref[...].astype(F32)
    t, s = position_masks()
    since = summed(s <= t, ghi, glo)
    until = summed(s > t, ghi, glo)
    kept = k32 * jnp.exp(until)
    q_ref[...] = q_ref[...] * jnp.asarray(DK**-0.5, BF16)
    head = lax.broadcasted_iota(jnp.int32, (ROWS, HEADS * DK), 1) // DK
    state = jnp.zeros((DV, HEADS * DK), F32)
    for h in range(HEADS):
        state += lax.dot_general(
            v_ref[:, h * DV : (h + 1) * DV],
            jnp.where(head == h, kept, 0.0).astype(BF16),
            (((0,), (0,)), ((), ())),
            preferred_element_type=F32,
        )
    state_ref[:DV, :] = state
    state_ref[DV:, :] = jnp.broadcast_to(since[ROWS - 1 :, :], (8, HEADS * DK))


def inside_kernel(q_ref, k_ref, v_ref, ghi_ref, glo_ref, mixed_ref, scores):
    q32 = q_ref[...].astype(F32)
    k32 = k_ref[...].astype(F32)
    head = lax.broadcasted_iota(jnp.int32, (ROWS, HEADS * DK), 1) // DK
    t, s = position_masks()

    def products(qs, ks):
        stacked = jnp.concatenate([jnp.where(head == h, qs, 0.0).astype(BF16) for h in range(HEADS)], axis=0)
        return dot_t(stacked, ks.astype(BF16))

    same = products(q32, k32)
    for h in range(HEADS):
        rows = pl.ds(h * ROWS, ROWS)
        scores[rows, :] = jnp.where(t == s, same[h * ROWS : (h + 1) * ROWS], 0.0)

    @pl.loop(0, LEVELS)
    def _(n):
        tn, sn = t >> n, s >> n
        upper = (tn & 1) == 1
        gap = summed((tn == sn) & ((upper & (s <= t)) | (~upper & (s > t))), ghi_ref[...], glo_ref[...])
        scale = jnp.exp(gap)
        part = products(q32 * scale, k32 * scale)
        chosen = upper & (tn == sn + 1)
        for h in range(HEADS):
            rows = pl.ds(h * ROWS, ROWS)
            scores[rows, :] = jnp.where(chosen, part[h * ROWS : (h + 1) * ROWS], scores[rows, :])

    for h in range(HEADS):
        columns = pl.ds(h * DV, DV)
        mixed_ref[:, columns] = jnp.dot(
            scores[pl.ds(h * ROWS, ROWS), :].astype(BF16), v_ref[:, columns], preferred_element_type=F32
        )


def output_kernel(
    place_ref, mixed_ref, q_ref, ghi_ref, glo_ref, outgate_ref, gain_ref, s1_ref, s2_ref, s3_ref, *refs
):
    (out_ref,) = refs[4:]
    states = [
        pltpu.roll(ref[...], (HEADS - back) * DK, axis=1) for back, ref in ((1, s1_ref), (2, s2_ref), (3, s3_ref))
    ]
    decay = [s[DV : DV + 1, :] for s in states]
    entering = (
        states[0][:DV]
        + jnp.exp(decay[0]) * states[1][:DV]
        + jnp.exp(decay[0] + decay[1]) * states[2][:DV]
    ).astype(BF16)
    t, s = position_masks()
    since = summed(s <= t, ghi_ref[...], glo_ref[...])
    scaled = q_ref[...].astype(F32) * jnp.exp(since)
    head = lax.broadcasted_iota(jnp.int32, (ROWS, HEADS * DK), 1) // DK
    gated = []
    for h in range(HEADS):
        columns = pl.ds(h * DV, DV)
        mixed = mixed_ref[:, columns] + dot_t(jnp.where(head == h, scaled, 0.0).astype(BF16), entering)
        size = jnp.mean(mixed * mixed, -1, keepdims=True)
        opened = outgate_ref[:, columns].astype(F32)
        opened = opened / (1.0 + jnp.exp(-opened))
        gated.append((mixed * lax.rsqrt(size + HEAD_EPS) * gain_ref[...] * opened).astype(BF16))
    channels = jnp.concatenate(gated, axis=1)

    def store(columns, value):
        out_ref[:, columns] = value

    projected(place_ref, lambda: channels, lambda dz, y, dx: refs[dz][y, dx, TAIL:], store)


def call(kernel, outs, scalars, arrays, scratch=(), flops=1_000_000, space=pltpu.VMEM):
    if space != pltpu.VMEM:
        arrays = [pltpu.with_memory_space_constraint(array, space) for array in arrays]
    in_specs = [pl.BlockSpec(memory_space=pltpu.SMEM)] * len(scalars) + [
        pl.BlockSpec(memory_space=space)
    ] * len(arrays)
    return pl.pallas_call(
        kernel,
        out_shape=[jax.ShapeDtypeStruct(*out) for out in outs],
        in_specs=in_specs,
        out_specs=[pl.BlockSpec(memory_space=pltpu.VMEM)] * len(outs),
        scratch_shapes=scratch,
        compiler_params=pltpu.CompilerParams(vmem_limit_bytes=VMEM_LIMIT),
        cost_estimate=pl.CostEstimate(flops=flops, bytes_accessed=1_000_000, transcendentals=0),
    )(*scalars, *arrays)


def on_device(
    stream,
    gate_weight,
    up_weight,
    down_weight,
    query_weight,
    key_weight,
    value_weight,
    outgate_weight,
    decay_down,
    decay_up,
    decay_bias,
    head_gain,
    out_weight,
    norm_gain,
):
    core = lax.axis_index("c")
    place = jnp.stack([lax.axis_index("z"), lax.axis_index("x"), core]).astype(jnp.int32)

    def swapped(value):
        return lax.ppermute(value, "c", [(0, 1), (1, 0)])

    other = swapped(stream)
    rows = jnp.where(core == 0, jnp.concatenate([stream, other]), jnp.concatenate([other, stream]))

    large, small = call(
        prepare_kernel,
        [((2 * HID + MIX, LANE), BF16), ((HID + TAIL + DV, LANE), BF16)],
        [],
        [
            gate_weight.T,
            up_weight.T,
            query_weight.T,
            key_weight.T,
            value_weight,
            outgate_weight,
            down_weight,
            out_weight,
        ],
        [pltpu.VMEM((LANE, DV), BF16), pltpu.VMEM((LANE, DV), BF16), pltpu.SemaphoreType.DMA((8,))],
        space=pltpu.HBM,
    )
    flat_ffn, flat_mix = [], []
    for shard, orders, units in ((small, SMALL, HID), (large, LARGE, 2 * HID)):
        planes = gathered_planes(shard, orders)
        rest = shard.shape[0] - units
        half = ((2, 4, units, LANE), BF16)
        (low,) = call(divide_low_kernel, [half], [], planes[:2])
        high, mix = call(divide_high_kernel, [half, ((4, 4, rest, LANE), BF16)], [], planes)
        flat_ffn = gathered_ring(low, high, last_of(orders)) + flat_ffn
        flat_mix = gathered_direct(mix, last_of(orders)) + flat_mix
    decay = jnp.concatenate(
        [decay_up.astype(F32), decay_bias[None, :], jnp.zeros((7, DK), F32)], axis=0
    )
    shifts = [shifted(decay, "yy", k) for k in (1, 2, 3)]
    decay = jnp.concatenate([decay, *shifts], axis=1)

    rows, decay_rows, decay_bias_row = lax.optimization_barrier((rows, decay[:32].astype(BF16), decay[32:33]))
    part, large = call(
        ffn_first_kernel,
        [((ROWS, D), BF16), ((4, 4, 4, 2 * HID, LANE), BF16)],
        [place],
        [rows, *flat_ffn],
        FFN_SCRATCH,
        4_400_000_000,
    )
    wide = ((ROWS, HEADS * DK), BF16)
    broad = ((ROWS, HEADS * DV), BF16)
    first, query, keys, values, outgate, ghi, glo, state = call(
        project_kernel,
        [((ROWS, D), BF16), wide, wide, broad, broad, wide, wide, ((DV + 8, HEADS * DK), F32)],
        [place],
        [
            rows,
            part,
            swapped(part),
            norm_gain[0:1],
            decay_down.T,
            decay_rows,
            decay_bias_row,
            *flat_mix,
        ],
        [pltpu.VMEM((4, ROWS, MIX + TAIL), BF16), pltpu.VMEM((4, 4, MIX, LANE), BF16)],
        2_000_000_000,
    )
    earlier = [
        lax.ppermute(state, "y", [(i, i + back) for i in range(4 - back)]) for back in (1, 2, 3)
    ]
    (mixed,) = call(
        inside_kernel,
        [((ROWS, HEADS * DV), F32)],
        [],
        [query, keys, values, ghi, glo],
        [pltpu.VMEM((HEADS * ROWS, ROWS), F32)],
        4_000_000_000,
    )
    (part,) = call(
        output_kernel,
        [((ROWS, D), BF16)],
        [place],
        [mixed, query, ghi, glo, outgate, head_gain[None, :], *earlier, *flat_mix[4:]],
        (),
        1_000_000_000,
    )
    own, keep, give = call(
        ffn_second_kernel,
        [((128, D), BF16)] * 3,
        [place],
        [first, part, swapped(part), norm_gain[1:2], large, *flat_ffn[8:]],
        [*FFN_SCRATCH, pltpu.VMEM((ROWS, D), BF16)],
        4_400_000_000,
    )
    (out,) = call(last_norm_kernel, [((128, D), BF16)], [], [own, keep, swapped(give), norm_gain[2:3]])
    return out


def solution(mesh):
    fine = Mesh(mesh.devices.reshape(2, 4, 4, 4, 2), ("r", "z", "x", "y", "c"))
    fs, tp = ("z", "x"), ("y", "c")
    in_specs = (
        P(("r", *fs, *tp), None),
        P(fs, tp),
        P(fs, tp),
        P(tp, fs),
        P(fs, tp),
        P(fs, tp),
        P(fs, tp),
        P(fs, tp),
        P(),
        P(None, tp),
        P(tp),
        P(),
        P(tp, fs),
        P(),
    )
    return jax.shard_map(on_device, mesh=fine, in_specs=in_specs, out_specs=P(("r", *fs, *tp), None), check_vma=False)
```

```python
import jax
import jax.numpy as jnp
import numpy as np
from jax import lax
from jax.experimental import pallas as pl
from jax.experimental.pallas import tpu as pltpu
from jax.sharding import Mesh, PartitionSpec as P


DK = 64
DV = 128
ROWS = 256
D = 2048
HID = 352
LANE = 128
HEADS = 4
MIX = 352
TAIL = 32
LEVELS = 8

RESIDUAL_SCALE = 2.0**0.5
BRANCH_SCALE = 0.5
NORM_EPS = 1e-05
HEAD_EPS = 0.01
GATE_DIVISOR = 16.0

F32 = jnp.float32
BF16 = jnp.bfloat16
LARGE = ("yxz", "zyx")
SMALL = ("xzy", "xzy")
NEAR = (0, 1, 3)
FAR = (2,)
AXES = {"r": 2, "z": 4, "x": 4, "y": 4, "c": 2}
VMEM_LIMIT = 20 * 1024 * 1024


def shifted(value, axes, step):
    pairs = []
    for n in range(256):
        r, z, x, y, c = (int(i) for i in np.unravel_index(n, tuple(AXES.values())))
        axis = axes[c]
        if axis == "z":
            ring = 4 * r + z
            go = -step if step == 2 and ring % 2 else step
            r, z = divmod((ring - go) % 8, 4)
        elif axis == "x":
            x = (x - step) % 4
        else:
            y = (y - step) % 4
        pairs.append((n, int(np.ravel_multi_index((r, z, x, y, c), tuple(AXES.values())))))
    return lax.ppermute(value, tuple(AXES), pairs)


def gathered_direct(value, axis):
    ahead, behind = shifted(value, axis, 1), shifted(value, axis, -1)
    return [value, ahead, shifted(value, axis, 2), behind]


def gathered_ring(low, high, axis):
    ahead_low, behind_low = shifted(low, axis, 1), shifted(low, axis, -1)
    behind_high, ahead_high = shifted(high, axis, -1), shifted(high, axis, 1)
    far_low = shifted(ahead_low, axis, 1)
    far_high = shifted(behind_high, axis, -1)
    return [low, high, ahead_low, ahead_high, far_low, far_high, behind_low, behind_high]


def gathered_planes(value, orders):
    first, second, _ = zip(*orders)
    line = gathered_direct(value, first)
    line = call(stack_kernel, [((4, *value.shape), BF16)], [], line)[0]
    return gathered_direct(line, second)


def last_of(orders):
    return tuple(order[2] for order in orders)


def fs_block(place_ref, dz, dx):
    return ((place_ref[0] + dz) % 4) * 4 + (place_ref[1] + dx) % 4


def normed(values, gain):
    average = jnp.mean(values, -1, keepdims=True)
    centred = values - average
    spread = jnp.mean(centred * centred, -1, keepdims=True)
    return (centred * lax.rsqrt(spread + NORM_EPS) * gain).astype(BF16)


def after_branch(out_ref, base_ref, mine_ref, other_ref, gain_ref, scale):
    @pl.loop(0, out_ref.shape[0] // 64)
    def _(n):
        rows = pl.ds(pl.multiple_of(n * 64, 64), 64)
        branch = mine_ref[rows, :].astype(F32) + other_ref[rows, :].astype(F32)
        out_ref[rows, :] = normed(RESIDUAL_SCALE * base_ref[rows, :].astype(F32) + scale * branch, gain_ref[...])


def dot_t(a, b):
    return lax.dot_general(a, b, (((1,), (1,)), ((), ())), preferred_element_type=F32)


def block_offsets(place_ref, i, j):
    core = place_ref[2]
    return i + core * (j - i), j + core * (i - j)


def ordered_columns(place_ref, ref, outer):
    blocks = []
    for i in outer:
        for j in range(4):
            column = fs_block(place_ref, *block_offsets(place_ref, i, j)) * LANE
            blocks.append(ref[:, pl.ds(pl.multiple_of(column, LANE), LANE)])
    return jnp.concatenate(blocks, axis=1)


def joined_features(block, outer):
    return jnp.concatenate([block(i, j) for i in outer for j in range(4)], axis=1)


def prepare_kernel(gate_ref, up_ref, query_ref, key_ref, value_ref, outgate_ref, down_ref, out_ref, *refs):
    large, small, value, outgate, sem = refs
    row, copies = 0, []
    for ref in (gate_ref, up_ref, query_ref, key_ref):
        copies.append((ref, large.at[pl.ds(row, ref.shape[0])]))
        row += ref.shape[0]
    copies += [(down_ref, small.at[pl.ds(0, HID)]), (out_ref, small.at[pl.ds(HID + TAIL, DV)])]
    copies += [(value_ref, value), (outgate_ref, outgate)]
    copies = [pltpu.make_async_copy(*pair, sem.at[n]) for n, pair in enumerate(copies)]
    for copy in copies:
        copy.start()
    for copy in copies:
        copy.wait()
    large[row : row + DV, :] = value[...].astype(F32).T.astype(BF16)
    turned = outgate[...].astype(F32).T.astype(BF16)
    large[row + DV :, :] = turned[: DV - TAIL]
    small[HID : HID + TAIL, :] = turned[DV - TAIL :]


def stack_kernel(*refs):
    for n in range(4):
        refs[4][n] = refs[n][...]


def divide_low_kernel(plane, ahead, low):
    units = low.shape[2]
    low[0] = plane[:, :units]
    low[1] = ahead[:, :units]


def divide_high_kernel(*refs):
    planes, (high, mix) = refs[:4], refs[4:]
    units = high.shape[2]
    for n, plane in enumerate(planes):
        if n > 1:
            high[n - 2] = plane[:, :units]
        mix[n] = plane[:, units:]


def arranged(place_ref, piece, y, dst):
    halves = len(piece)
    inner = 4 // halves
    for half, ref in enumerate(piece):

        @pl.when(place_ref[2] == 0)
        def _():
            @pl.loop(0, inner)
            def _(n):
                dst[half * inner + n] = ref[n, y]

        @pl.when((place_ref[2] == 1) & (y >= half * inner) & (y < (half + 1) * inner))
        def _():
            @pl.loop(0, 4)
            def _(n):
                dst[n] = ref[y - half * inner, n]


def gated_units(both):
    gate, upward = both[:, :HID], both[:, HID:]
    return (gate / (1.0 + jnp.exp(-gate)) * upward).astype(BF16)


def projected(place_ref, units, block, store):
    @pl.loop(0, 4)
    def _(dx):
        columns = [jnp.concatenate([block(dz, y, dx) for y in range(4)], axis=0) for dz in range(4)]
        part = jnp.dot(units(), jnp.concatenate(columns, axis=1), preferred_element_type=F32).astype(BF16)
        for dz in range(4):
            column = pl.multiple_of(fs_block(place_ref, dz, dx) * LANE, LANE)
            store(pl.ds(column, LANE), part[:, dz * LANE : (dz + 1) * LANE])


def ffn_early_kernel(place_ref, x_ref, *refs):
    near_ref, part_ref = refs[6:]
    x = ordered_columns(place_ref, x_ref, NEAR)

    @pl.loop(0, 4)
    def _(y):
        for n in range(3):
            arranged(place_ref, refs[2 * n : 2 * n + 2], y, near_ref.at[y, n])
        part_ref[y] = dot_t(x, joined_features(lambda n, j: near_ref[y, n, j], range(3)))


def ffn_late_kernel(place_ref, x_ref, part_ref, *refs):
    small_p = refs[2:10]
    out_ref, far_ref, hidden = refs[10:]
    x = ordered_columns(place_ref, x_ref, FAR)

    @pl.loop(0, 4)
    def _(y):
        arranged(place_ref, refs[:2], y, far_ref.at[y])
        hidden[y] = gated_units(part_ref[y] + dot_t(x, joined_features(lambda i, j: far_ref[y, j], FAR)))

    def store(columns, value):
        out_ref[:, columns] = value

    projected(
        place_ref,
        lambda: jnp.concatenate([hidden[y] for y in range(4)], axis=1),
        lambda dz, y, dx: small_p[2 * y + dz // 2][dz % 2, dx],
        store,
    )


def ffn_second_kernel(place_ref, base_ref, mine_ref, other_ref, gain_ref, near_ref, far_ref, *refs):
    small_p = refs[:8]
    own_ref, keep_ref, give_ref, hidden, second = refs[8:]
    core = place_ref[2]
    after_branch(second, base_ref, mine_ref, other_ref, gain_ref, 1.0)
    own_ref[...] = second[pl.ds(pl.multiple_of(core * 128, 128), 128), :]
    x = ordered_columns(place_ref, second, NEAR + FAR)

    @pl.loop(0, 4)
    def _(y):
        rows = joined_features(lambda n, j: far_ref[y, j] if n == 3 else near_ref[y, n, j], range(4))
        hidden[y] = gated_units(dot_t(x, rows))

    def store(columns, value):
        keep_ref[:, columns] = jnp.where(core == 0, value[:128], value[128:])
        give_ref[:, columns] = jnp.where(core == 0, value[128:], value[:128])

    projected(
        place_ref,
        lambda: jnp.concatenate([hidden[y] for y in range(4)], axis=1),
        lambda dz, y, dx: small_p[2 * y + dz // 2][dz % 2, dx],
        store,
    )


def last_norm_kernel(base_ref, mine_ref, other_ref, gain_ref, out_ref):
    after_branch(out_ref, base_ref, mine_ref, other_ref, gain_ref, BRANCH_SCALE)


FFN_SCRATCH = (pltpu.VMEM((4, ROWS, HID), BF16),)


def position_masks():
    t = lax.broadcasted_iota(jnp.int32, (ROWS, ROWS), 0)
    s = lax.broadcasted_iota(jnp.int32, (ROWS, ROWS), 1)
    return t, s


def summed(mask, high, low):
    ones = jnp.where(mask, 1.0, 0.0).astype(BF16)
    return jnp.dot(ones, high, preferred_element_type=F32) + jnp.dot(ones, low, preferred_element_type=F32)


def project_kernel(place_ref, base_ref, mine_ref, other_ref, gain_ref, down_ref, up_ref, bias_ref, *refs):
    first_ref, q_ref, k_ref, v_ref, outgate_ref, ghi_ref, glo_ref, state_ref, parts, large, tails = refs[8:]
    large_p, small_p = refs[:4], refs[4:8]
    after_branch(first_ref, base_ref, mine_ref, other_ref, gain_ref, BRANCH_SCALE)
    first = first_ref[...]
    low = dot_t(first, down_ref[...]).astype(BF16)
    pre = jnp.dot(low, up_ref[...], preferred_element_type=F32) + bias_ref[...]
    log_gate = (jnp.minimum(pre, 0.0) - jnp.log1p(jnp.exp(-jnp.abs(pre)))) / GATE_DIVISOR
    ghi = log_gate.astype(BF16)
    glo = (log_gate - ghi.astype(F32)).astype(BF16)
    ghi_ref[...] = ghi
    glo_ref[...] = glo
    x = ordered_columns(place_ref, first_ref, range(4))

    @pl.loop(0, 4)
    def _(y):
        for n in range(4):
            arranged(place_ref, large_p[n : n + 1], y, large.at[n])

            @pl.when(y == n)
            def _():
                @pl.loop(0, 4)
                def _(i):
                    for j in range(4):
                        dz, dx = block_offsets(place_ref, i, j)
                        tails[i, j] = small_p[n][dz, dx, :TAIL]

        rows = [
            joined_features(lambda i, j: large[i, j], range(4)),
            joined_features(lambda i, j: tails[i, j], range(4)),
        ]
        parts[y] = dot_t(x, jnp.concatenate(rows, axis=0)).astype(BF16)

    queries, keys = [], []
    for y in range(4):
        queries.append(parts[y, :, :DK])
        keys.append(parts[y, :, DK : 2 * DK])
        v_ref[:, pl.ds(y * DV, DV)] = parts[y, :, 2 * DK : 2 * DK + DV]
        outgate_ref[:, pl.ds(y * DV, DV)] = parts[y, :, 2 * DK + DV :]
    q_ref[...] = jnp.concatenate(queries, axis=1)
    k_ref[...] = jnp.concatenate(keys, axis=1)
    k32 = k_ref[...].astype(F32)
    t, s = position_masks()
    since = summed(s <= t, ghi, glo)
    until = summed(s > t, ghi, glo)
    kept = k32 * jnp.exp(until)
    q_ref[...] = q_ref[...] * jnp.asarray(DK**-0.5, BF16)
    head = lax.broadcasted_iota(jnp.int32, (ROWS, HEADS * DK), 1) // DK
    state = jnp.zeros((DV, HEADS * DK), F32)
    for h in range(HEADS):
        state += lax.dot_general(
            v_ref[:, h * DV : (h + 1) * DV],
            jnp.where(head == h, kept, 0.0).astype(BF16),
            (((0,), (0,)), ((), ())),
            preferred_element_type=F32,
        )
    state_ref[:DV, :] = state
    state_ref[DV:, :] = jnp.broadcast_to(since[ROWS - 1 :, :], (8, HEADS * DK))


def inside_kernel(q_ref, k_ref, v_ref, ghi_ref, glo_ref, mixed_ref, scores):
    q32 = q_ref[...].astype(F32)
    k32 = k_ref[...].astype(F32)
    head = lax.broadcasted_iota(jnp.int32, (ROWS, HEADS * DK), 1) // DK
    t, s = position_masks()

    def products(qs, ks):
        stacked = jnp.concatenate([jnp.where(head == h, qs, 0.0).astype(BF16) for h in range(HEADS)], axis=0)
        return dot_t(stacked, ks.astype(BF16))

    same = products(q32, k32)
    for h in range(HEADS):
        rows = pl.ds(h * ROWS, ROWS)
        scores[rows, :] = jnp.where(t == s, same[h * ROWS : (h + 1) * ROWS], 0.0)

    @pl.loop(0, LEVELS)
    def _(n):
        tn, sn = t >> n, s >> n
        upper = (tn & 1) == 1
        gap = summed((tn == sn) & ((upper & (s <= t)) | (~upper & (s > t))), ghi_ref[...], glo_ref[...])
        scale = jnp.exp(gap)
        part = products(q32 * scale, k32 * scale)
        chosen = upper & (tn == sn + 1)
        for h in range(HEADS):
            rows = pl.ds(h * ROWS, ROWS)
            scores[rows, :] = jnp.where(chosen, part[h * ROWS : (h + 1) * ROWS], scores[rows, :])

    for h in range(HEADS):
        columns = pl.ds(h * DV, DV)
        mixed_ref[:, columns] = jnp.dot(
            scores[pl.ds(h * ROWS, ROWS), :].astype(BF16), v_ref[:, columns], preferred_element_type=F32
        )


def output_kernel(
    place_ref, mixed_ref, q_ref, ghi_ref, glo_ref, outgate_ref, gain_ref, s1_ref, s2_ref, s3_ref, *refs
):
    (out_ref,) = refs[4:]
    states = [
        pltpu.roll(ref[...], (HEADS - back) * DK, axis=1) for back, ref in ((1, s1_ref), (2, s2_ref), (3, s3_ref))
    ]
    decay = [s[DV : DV + 1, :] for s in states]
    entering = (
        states[0][:DV]
        + jnp.exp(decay[0]) * states[1][:DV]
        + jnp.exp(decay[0] + decay[1]) * states[2][:DV]
    ).astype(BF16)
    t, s = position_masks()
    since = summed(s <= t, ghi_ref[...], glo_ref[...])
    scaled = q_ref[...].astype(F32) * jnp.exp(since)
    head = lax.broadcasted_iota(jnp.int32, (ROWS, HEADS * DK), 1) // DK
    gated = []
    for h in range(HEADS):
        columns = pl.ds(h * DV, DV)
        mixed = mixed_ref[:, columns] + dot_t(jnp.where(head == h, scaled, 0.0).astype(BF16), entering)
        size = jnp.mean(mixed * mixed, -1, keepdims=True)
        opened = outgate_ref[:, columns].astype(F32)
        opened = opened / (1.0 + jnp.exp(-opened))
        gated.append((mixed * lax.rsqrt(size + HEAD_EPS) * gain_ref[...] * opened).astype(BF16))
    channels = jnp.concatenate(gated, axis=1)

    def store(columns, value):
        out_ref[:, columns] = value

    projected(place_ref, lambda: channels, lambda dz, y, dx: refs[y][dz, dx, TAIL:], store)


def call(kernel, outs, scalars, arrays, scratch=(), flops=1_000_000, space=pltpu.VMEM):
    if space != pltpu.VMEM:
        arrays = [pltpu.with_memory_space_constraint(array, space) for array in arrays]
    in_specs = [pl.BlockSpec(memory_space=pltpu.SMEM)] * len(scalars) + [
        pl.BlockSpec(memory_space=space)
    ] * len(arrays)
    return pl.pallas_call(
        kernel,
        out_shape=[jax.ShapeDtypeStruct(*out) for out in outs],
        in_specs=in_specs,
        out_specs=[pl.BlockSpec(memory_space=pltpu.VMEM)] * len(outs),
        scratch_shapes=scratch,
        compiler_params=pltpu.CompilerParams(vmem_limit_bytes=VMEM_LIMIT),
        cost_estimate=pl.CostEstimate(flops=flops, bytes_accessed=1_000_000, transcendentals=0),
    )(*scalars, *arrays)


def on_device(
    stream,
    gate_weight,
    up_weight,
    down_weight,
    query_weight,
    key_weight,
    value_weight,
    outgate_weight,
    decay_down,
    decay_up,
    decay_bias,
    head_gain,
    out_weight,
    norm_gain,
):
    core = lax.axis_index("c")
    place = jnp.stack([lax.axis_index("z"), lax.axis_index("x"), core]).astype(jnp.int32)

    def swapped(value):
        return lax.ppermute(value, "c", [(0, 1), (1, 0)])

    other = swapped(stream)
    rows = jnp.where(core == 0, jnp.concatenate([stream, other]), jnp.concatenate([other, stream]))

    large, small = call(
        prepare_kernel,
        [((2 * HID + MIX, LANE), BF16), ((HID + TAIL + DV, LANE), BF16)],
        [],
        [
            gate_weight.T,
            up_weight.T,
            query_weight.T,
            key_weight.T,
            value_weight,
            outgate_weight,
            down_weight,
            out_weight,
        ],
        [pltpu.VMEM((LANE, DV), BF16), pltpu.VMEM((LANE, DV), BF16), pltpu.SemaphoreType.DMA((8,))],
        space=pltpu.HBM,
    )
    flat_ffn, flat_mix = [], []
    for shard, orders, units in ((small, SMALL, HID), (large, LARGE, 2 * HID)):
        planes = gathered_planes(shard, orders)
        rest = shard.shape[0] - units
        half = ((2, 4, units, LANE), BF16)
        (low,) = call(divide_low_kernel, [half], [], planes[:2])
        high, mix = call(divide_high_kernel, [half, ((4, 4, rest, LANE), BF16)], [], planes)
        flat_ffn = gathered_ring(low, high, last_of(orders)) + flat_ffn
        flat_mix = gathered_direct(mix, last_of(orders)) + flat_mix
    decay = jnp.concatenate(
        [decay_up.astype(F32), decay_bias[None, :], jnp.zeros((7, DK), F32)], axis=0
    )
    shifts = [shifted(decay, "yy", k) for k in (1, 2, 3)]
    decay = jnp.concatenate([decay, *shifts], axis=1)

    rows, decay_rows, decay_bias_row = lax.optimization_barrier((rows, decay[:32].astype(BF16), decay[32:33]))
    large_p, small_p = flat_ffn[:8], flat_ffn[8:]
    near, part = call(
        ffn_early_kernel,
        [((4, 3, 4, 2 * HID, LANE), BF16), ((4, ROWS, 2 * HID), F32)],
        [place],
        [rows, *large_p[:4], *large_p[6:]],
        (),
        2_200_000_000,
    )
    part, far = call(
        ffn_late_kernel,
        [((ROWS, D), BF16), ((4, 4, 2 * HID, LANE), BF16)],
        [place],
        [rows, part, *large_p[4:6], *small_p],
        FFN_SCRATCH,
        2_200_000_000,
    )
    wide = ((ROWS, HEADS * DK), BF16)
    broad = ((ROWS, HEADS * DV), BF16)
    first, query, keys, values, outgate, ghi, glo, state = call(
        project_kernel,
        [((ROWS, D), BF16), wide, wide, broad, broad, wide, wide, ((DV + 8, HEADS * DK), F32)],
        [place],
        [
            rows,
            part,
            swapped(part),
            norm_gain[0:1],
            decay_down.T,
            decay_rows,
            decay_bias_row,
            *flat_mix,
        ],
        [pltpu.VMEM((4, ROWS, MIX + TAIL), BF16), pltpu.VMEM((4, 4, MIX, LANE), BF16), pltpu.VMEM((4, 4, TAIL, LANE), BF16)],
        2_000_000_000,
    )
    earlier = [
        lax.ppermute(state, "y", [(i, i + back) for i in range(4 - back)]) for back in (1, 2, 3)
    ]
    (mixed,) = call(
        inside_kernel,
        [((ROWS, HEADS * DV), F32)],
        [],
        [query, keys, values, ghi, glo],
        [pltpu.VMEM((HEADS * ROWS, ROWS), F32)],
        4_000_000_000,
    )
    (part,) = call(
        output_kernel,
        [((ROWS, D), BF16)],
        [place],
        [mixed, query, ghi, glo, outgate, head_gain[None, :], *earlier, *flat_mix[4:]],
        (),
        1_000_000_000,
    )
    own, keep, give = call(
        ffn_second_kernel,
        [((128, D), BF16)] * 3,
        [place],
        [first, part, swapped(part), norm_gain[1:2], near, far, *small_p],
        [*FFN_SCRATCH, pltpu.VMEM((ROWS, D), BF16)],
        4_400_000_000,
    )
    (out,) = call(last_norm_kernel, [((128, D), BF16)], [], [own, keep, swapped(give), norm_gain[2:3]])
    return out


def solution(mesh):
    fine = Mesh(mesh.devices.reshape(2, 4, 4, 4, 2), ("r", "z", "x", "y", "c"))
    fs, tp = ("z", "x"), ("y", "c")
    in_specs = (
        P(("r", *fs, *tp), None),
        P(fs, tp),
        P(fs, tp),
        P(tp, fs),
        P(fs, tp),
        P(fs, tp),
        P(fs, tp),
        P(fs, tp),
        P(),
        P(None, tp),
        P(tp),
        P(),
        P(tp, fs),
        P(),
    )
    return jax.shard_map(on_device, mesh=fine, in_specs=in_specs, out_specs=P(("r", *fs, *tp), None), check_vma=False)
```

```python
import jax
import jax.numpy as jnp
import numpy as np
from jax import lax
from jax.experimental import pallas as pl
from jax.experimental.pallas import tpu as pltpu
from jax.sharding import Mesh, PartitionSpec as P


DK = 64
DV = 128
ROWS = 256
D = 2048
HID = 352
LANE = 128
HEADS = 4
MIX = 176
TAIL = 80
LEVELS = 8

RESIDUAL_SCALE = 2.0**0.5
BRANCH_SCALE = 0.5
NORM_EPS = 1e-05
HEAD_EPS = 0.01
GATE_DIVISOR = 16.0

F32 = jnp.float32
BF16 = jnp.bfloat16
LARGE = ("yxz", "zyx")
SMALL = ("xzy", "xzy")
NEAR = (0, 1, 3)
FAR = (2,)
AXES = {"r": 2, "z": 4, "x": 4, "y": 4, "c": 2}
VMEM_LIMIT = 20 * 1024 * 1024


def shifted(value, axes, step):
    pairs = []
    for n in range(256):
        r, z, x, y, c = (int(i) for i in np.unravel_index(n, tuple(AXES.values())))
        axis = axes[c]
        if axis == "z":
            ring = 4 * r + z
            go = -step if step == 2 and ring % 2 else step
            r, z = divmod((ring - go) % 8, 4)
        elif axis == "x":
            x = (x - step) % 4
        else:
            y = (y - step) % 4
        pairs.append((n, int(np.ravel_multi_index((r, z, x, y, c), tuple(AXES.values())))))
    return lax.ppermute(value, tuple(AXES), pairs)


def gathered_direct(value, axis):
    ahead, behind = shifted(value, axis, 1), shifted(value, axis, -1)
    return [value, ahead, shifted(value, axis, 2), behind]


def gathered_ring(low, high, axis):
    ahead_low, behind_low = shifted(low, axis, 1), shifted(low, axis, -1)
    behind_high, ahead_high = shifted(high, axis, -1), shifted(high, axis, 1)
    far_low = shifted(ahead_low, axis, 1)
    far_high = shifted(behind_high, axis, -1)
    return [low, high, ahead_low, ahead_high, far_low, far_high, behind_low, behind_high]


def gathered_planes(value, orders):
    first, second, _ = zip(*orders)
    line = gathered_direct(value, first)
    line = call(stack_kernel, [((4, *value.shape), BF16)], [], line)[0]
    return gathered_direct(line, second)


def last_of(orders):
    return tuple(order[2] for order in orders)


def fs_block(place_ref, dz, dx):
    return ((place_ref[0] + dz) % 4) * 4 + (place_ref[1] + dx) % 4


def normed(values, gain):
    average = jnp.mean(values, -1, keepdims=True)
    centred = values - average
    spread = jnp.mean(centred * centred, -1, keepdims=True)
    return (centred * lax.rsqrt(spread + NORM_EPS) * gain).astype(BF16)


def after_branch(out_ref, base_ref, mine_ref, other_ref, gain_ref, scale):
    @pl.loop(0, out_ref.shape[0] // 64)
    def _(n):
        rows = pl.ds(pl.multiple_of(n * 64, 64), 64)
        branch = mine_ref[rows, :].astype(F32) + other_ref[rows, :].astype(F32)
        out_ref[rows, :] = normed(RESIDUAL_SCALE * base_ref[rows, :].astype(F32) + scale * branch, gain_ref[...])


def dot_t(a, b):
    return lax.dot_general(a, b, (((1,), (1,)), ((), ())), preferred_element_type=F32)


def block_offsets(place_ref, i, j):
    core = place_ref[2]
    return i + core * (j - i), j + core * (i - j)


def ordered_columns(place_ref, ref, outer):
    blocks = []
    for i in outer:
        for j in range(4):
            column = fs_block(place_ref, *block_offsets(place_ref, i, j)) * LANE
            blocks.append(ref[:, pl.ds(pl.multiple_of(column, LANE), LANE)])
    return jnp.concatenate(blocks, axis=1)


def joined_features(block, outer):
    return jnp.concatenate([block(i, j) for i in outer for j in range(4)], axis=1)


def prepare_kernel(gate_ref, up_ref, query_ref, key_ref, value_ref, outgate_ref, down_ref, out_ref, *refs):
    large, small, value, outgate, sem = refs
    row, copies = 0, []
    for ref in (gate_ref, up_ref, query_ref, key_ref):
        copies.append((ref, large.at[pl.ds(row, ref.shape[0])]))
        row += ref.shape[0]
    cut = DV - TAIL
    copies += [(down_ref, small.at[pl.ds(0, HID)]), (out_ref.at[pl.ds(0, cut)], large.at[pl.ds(2 * HID + MIX + DV, cut)])]
    copies += [(out_ref.at[pl.ds(cut, TAIL)], small.at[pl.ds(HID + TAIL, TAIL)])]
    copies += [(value_ref, value), (outgate_ref, outgate)]
    copies = [pltpu.make_async_copy(*pair, sem.at[n]) for n, pair in enumerate(copies)]
    for copy in copies:
        copy.start()
    for copy in copies:
        copy.wait()
    turned = value[...].astype(F32).T.astype(BF16)
    large[row : row + cut, :] = turned[:cut]
    small[HID : HID + TAIL, :] = turned[cut:]
    large[row + cut : row + cut + DV, :] = outgate[...].astype(F32).T.astype(BF16)


def stack_kernel(*refs):
    for n in range(4):
        refs[4][n] = refs[n][...]


def divide_low_kernel(plane, ahead, low):
    units = low.shape[2]
    low[0] = plane[:, :units]
    low[1] = ahead[:, :units]


def divide_high_kernel(*refs):
    planes, (high, mix, rest) = refs[:4], refs[4:]
    units, rows = high.shape[2], mix.shape[2]
    for n, plane in enumerate(planes):
        if n > 1:
            high[n - 2] = plane[:, :units]
        mix[n] = plane[:, units : units + rows]
        rest[n] = plane[:, units + rows :]


def arranged(place_ref, piece, y, dst):
    halves = len(piece)
    inner = 4 // halves
    for half, ref in enumerate(piece):

        @pl.when(place_ref[2] == 0)
        def _():
            @pl.loop(0, inner)
            def _(n):
                dst[half * inner + n] = ref[n, y]

        @pl.when((place_ref[2] == 1) & (y >= half * inner) & (y < (half + 1) * inner))
        def _():
            @pl.loop(0, 4)
            def _(n):
                dst[n] = ref[y - half * inner, n]


def arranged_small(place_ref, pieces, y, dst):
    for n in range(4):

        @pl.when(y == n)
        def _():
            @pl.loop(0, 4)
            def _(i):
                for j in range(4):
                    dz, dx = block_offsets(place_ref, i, j)
                    dst[i, j] = pieces[n][dz, dx]


def gated_units(both):
    gate, upward = both[:, :HID], both[:, HID:]
    return (gate / (1.0 + jnp.exp(-gate)) * upward).astype(BF16)


def projected(place_ref, units, block, store):
    @pl.loop(0, 4)
    def _(dx):
        columns = [jnp.concatenate([block(dz, y, dx) for y in range(4)], axis=0) for dz in range(4)]
        part = jnp.dot(units(), jnp.concatenate(columns, axis=1), preferred_element_type=F32).astype(BF16)
        for dz in range(4):
            column = pl.multiple_of(fs_block(place_ref, dz, dx) * LANE, LANE)
            store(pl.ds(column, LANE), part[:, dz * LANE : (dz + 1) * LANE])


def ffn_early_kernel(place_ref, x_ref, *refs):
    near_ref, part_ref = refs[6:]
    x = ordered_columns(place_ref, x_ref, NEAR)

    @pl.loop(0, 4)
    def _(y):
        for n in range(3):
            arranged(place_ref, refs[2 * n : 2 * n + 2], y, near_ref.at[y, n])
        part_ref[y] = dot_t(x, joined_features(lambda n, j: near_ref[y, n, j], range(3)))


def ffn_late_kernel(place_ref, x_ref, part_ref, *refs):
    small_p = refs[2:10]
    out_ref, far_ref, hidden = refs[10:]
    x = ordered_columns(place_ref, x_ref, FAR)

    @pl.loop(0, 4)
    def _(y):
        arranged(place_ref, refs[:2], y, far_ref.at[y])
        hidden[y] = gated_units(part_ref[y] + dot_t(x, joined_features(lambda i, j: far_ref[y, j], FAR)))

    def store(columns, value):
        out_ref[:, columns] = value

    projected(
        place_ref,
        lambda: jnp.concatenate([hidden[y] for y in range(4)], axis=1),
        lambda dz, y, dx: small_p[2 * y + dz // 2][dz % 2, dx],
        store,
    )


def ffn_second_kernel(place_ref, base_ref, mine_ref, other_ref, gain_ref, near_ref, far_ref, *refs):
    small_p = refs[:8]
    own_ref, keep_ref, give_ref, hidden, second = refs[8:]
    core = place_ref[2]
    after_branch(second, base_ref, mine_ref, other_ref, gain_ref, 1.0)
    own_ref[...] = second[pl.ds(pl.multiple_of(core * 128, 128), 128), :]
    x = ordered_columns(place_ref, second, NEAR + FAR)

    @pl.loop(0, 4)
    def _(y):
        rows = joined_features(lambda n, j: far_ref[y, j] if n == 3 else near_ref[y, n, j], range(4))
        hidden[y] = gated_units(dot_t(x, rows))

    def store(columns, value):
        keep_ref[:, columns] = jnp.where(core == 0, value[:128], value[128:])
        give_ref[:, columns] = jnp.where(core == 0, value[128:], value[:128])

    projected(
        place_ref,
        lambda: jnp.concatenate([hidden[y] for y in range(4)], axis=1),
        lambda dz, y, dx: small_p[2 * y + dz // 2][dz % 2, dx],
        store,
    )


def last_norm_kernel(base_ref, mine_ref, other_ref, gain_ref, out_ref):
    after_branch(out_ref, base_ref, mine_ref, other_ref, gain_ref, BRANCH_SCALE)


FFN_SCRATCH = (pltpu.VMEM((4, ROWS, HID), BF16),)


def position_masks():
    t = lax.broadcasted_iota(jnp.int32, (ROWS, ROWS), 0)
    s = lax.broadcasted_iota(jnp.int32, (ROWS, ROWS), 1)
    return t, s


def summed(mask, high, low):
    ones = jnp.where(mask, 1.0, 0.0).astype(BF16)
    return jnp.dot(ones, high, preferred_element_type=F32) + jnp.dot(ones, low, preferred_element_type=F32)


def project_kernel(place_ref, base_ref, mine_ref, other_ref, gain_ref, down_ref, up_ref, bias_ref, *refs):
    first_ref, q_ref, k_ref, v_ref, ghi_ref, glo_ref, state_ref, parts, large, tails = refs[8:]
    large_p, small_p = refs[:4], refs[4:8]
    after_branch(first_ref, base_ref, mine_ref, other_ref, gain_ref, BRANCH_SCALE)
    first = first_ref[...]
    low = dot_t(first, down_ref[...]).astype(BF16)
    pre = jnp.dot(low, up_ref[...], preferred_element_type=F32) + bias_ref[...]
    log_gate = (jnp.minimum(pre, 0.0) - jnp.log1p(jnp.exp(-jnp.abs(pre)))) / GATE_DIVISOR
    ghi = log_gate.astype(BF16)
    glo = (log_gate - ghi.astype(F32)).astype(BF16)
    ghi_ref[...] = ghi
    glo_ref[...] = glo
    x = ordered_columns(place_ref, first_ref, range(4))

    @pl.loop(0, 4)
    def _(y):
        for n in range(4):
            arranged(place_ref, large_p[n : n + 1], y, large.at[n])

        arranged_small(place_ref, small_p, y, tails)
        rows = [
            joined_features(lambda i, j: large[i, j], range(4)),
            joined_features(lambda i, j: tails[i, j], range(4)),
        ]
        parts[y] = dot_t(x, jnp.concatenate(rows, axis=0)).astype(BF16)

    queries, keys = [], []
    for y in range(4):
        queries.append(parts[y, :, :DK])
        keys.append(parts[y, :, DK : 2 * DK])
        v_ref[:, pl.ds(y * DV, DV)] = parts[y, :, 2 * DK : 2 * DK + DV]
    q_ref[...] = jnp.concatenate(queries, axis=1)
    k_ref[...] = jnp.concatenate(keys, axis=1)
    k32 = k_ref[...].astype(F32)
    t, s = position_masks()
    since = summed(s <= t, ghi, glo)
    until = summed(s > t, ghi, glo)
    kept = k32 * jnp.exp(until)
    q_ref[...] = q_ref[...] * jnp.asarray(DK**-0.5, BF16)
    head = lax.broadcasted_iota(jnp.int32, (ROWS, HEADS * DK), 1) // DK
    state = jnp.zeros((DV, HEADS * DK), F32)
    for h in range(HEADS):
        state += lax.dot_general(
            v_ref[:, h * DV : (h + 1) * DV],
            jnp.where(head == h, kept, 0.0).astype(BF16),
            (((0,), (0,)), ((), ())),
            preferred_element_type=F32,
        )
    state_ref[:DV, :] = state
    state_ref[DV:, :] = jnp.broadcast_to(since[ROWS - 1 :, :], (8, HEADS * DK))


def inside_kernel(q_ref, k_ref, v_ref, ghi_ref, glo_ref, mixed_ref, scores):
    q32 = q_ref[...].astype(F32)
    k32 = k_ref[...].astype(F32)
    head = lax.broadcasted_iota(jnp.int32, (ROWS, HEADS * DK), 1) // DK
    t, s = position_masks()

    def products(qs, ks):
        stacked = jnp.concatenate([jnp.where(head == h, qs, 0.0).astype(BF16) for h in range(HEADS)], axis=0)
        return dot_t(stacked, ks.astype(BF16))

    same = products(q32, k32)
    for h in range(HEADS):
        rows = pl.ds(h * ROWS, ROWS)
        scores[rows, :] = jnp.where(t == s, same[h * ROWS : (h + 1) * ROWS], 0.0)

    @pl.loop(0, LEVELS)
    def _(n):
        tn, sn = t >> n, s >> n
        upper = (tn & 1) == 1
        gap = summed((tn == sn) & ((upper & (s <= t)) | (~upper & (s > t))), ghi_ref[...], glo_ref[...])
        scale = jnp.exp(gap)
        part = products(q32 * scale, k32 * scale)
        chosen = upper & (tn == sn + 1)
        for h in range(HEADS):
            rows = pl.ds(h * ROWS, ROWS)
            scores[rows, :] = jnp.where(chosen, part[h * ROWS : (h + 1) * ROWS], scores[rows, :])

    for h in range(HEADS):
        columns = pl.ds(h * DV, DV)
        mixed_ref[:, columns] = jnp.dot(
            scores[pl.ds(h * ROWS, ROWS), :].astype(BF16), v_ref[:, columns], preferred_element_type=F32
        )


def output_kernel(
    place_ref, mixed_ref, q_ref, ghi_ref, glo_ref, first_ref, gain_ref, s1_ref, s2_ref, s3_ref, *refs
):
    out_ref, large, small, outgate = refs[8:]
    x = ordered_columns(place_ref, first_ref, range(4))

    @pl.loop(0, 4)
    def _(y):
        for n in range(4):
            arranged(place_ref, refs[n : n + 1], y, large.at[y, n])
        arranged_small(place_ref, refs[4:8], y, small.at[y])
        outgate[y] = dot_t(x, joined_features(lambda i, j: large[y, i, j, :DV], range(4))).astype(BF16)

    states = [
        pltpu.roll(ref[...], (HEADS - back) * DK, axis=1) for back, ref in ((1, s1_ref), (2, s2_ref), (3, s3_ref))
    ]
    decay = [s[DV : DV + 1, :] for s in states]
    entering = (
        states[0][:DV]
        + jnp.exp(decay[0]) * states[1][:DV]
        + jnp.exp(decay[0] + decay[1]) * states[2][:DV]
    ).astype(BF16)
    t, s = position_masks()
    since = summed(s <= t, ghi_ref[...], glo_ref[...])
    scaled = q_ref[...].astype(F32) * jnp.exp(since)
    head = lax.broadcasted_iota(jnp.int32, (ROWS, HEADS * DK), 1) // DK
    gated = []
    for h in range(HEADS):
        columns = pl.ds(h * DV, DV)
        mixed = mixed_ref[:, columns] + dot_t(jnp.where(head == h, scaled, 0.0).astype(BF16), entering)
        size = jnp.mean(mixed * mixed, -1, keepdims=True)
        opened = outgate[h].astype(F32)
        opened = opened / (1.0 + jnp.exp(-opened))
        gated.append((mixed * lax.rsqrt(size + HEAD_EPS) * gain_ref[...] * opened).astype(BF16))
    channels = jnp.concatenate(gated, axis=1)

    @pl.loop(0, 4)
    def _(j):
        blocks = []
        for i in range(4):
            rows = [part for y in range(4) for part in (large[y, i, j, DV:], small[y, i, j])]
            blocks.append(jnp.concatenate(rows, axis=0))
        part = jnp.dot(channels, jnp.concatenate(blocks, axis=1), preferred_element_type=F32).astype(BF16)
        for i in range(4):
            column = pl.multiple_of(fs_block(place_ref, *block_offsets(place_ref, i, j)) * LANE, LANE)
            out_ref[:, pl.ds(column, LANE)] = part[:, i * LANE : (i + 1) * LANE]


def call(kernel, outs, scalars, arrays, scratch=(), flops=1_000_000, space=pltpu.VMEM):
    if space != pltpu.VMEM:
        arrays = [pltpu.with_memory_space_constraint(array, space) for array in arrays]
    in_specs = [pl.BlockSpec(memory_space=pltpu.SMEM)] * len(scalars) + [
        pl.BlockSpec(memory_space=space)
    ] * len(arrays)
    return pl.pallas_call(
        kernel,
        out_shape=[jax.ShapeDtypeStruct(*out) for out in outs],
        in_specs=in_specs,
        out_specs=[pl.BlockSpec(memory_space=pltpu.VMEM)] * len(outs),
        scratch_shapes=scratch,
        compiler_params=pltpu.CompilerParams(vmem_limit_bytes=VMEM_LIMIT),
        cost_estimate=pl.CostEstimate(flops=flops, bytes_accessed=1_000_000, transcendentals=0),
    )(*scalars, *arrays)


def on_device(
    stream,
    gate_weight,
    up_weight,
    down_weight,
    query_weight,
    key_weight,
    value_weight,
    outgate_weight,
    decay_down,
    decay_up,
    decay_bias,
    head_gain,
    out_weight,
    norm_gain,
):
    core = lax.axis_index("c")
    place = jnp.stack([lax.axis_index("z"), lax.axis_index("x"), core]).astype(jnp.int32)

    def swapped(value):
        return lax.ppermute(value, "c", [(0, 1), (1, 0)])

    other = swapped(stream)
    rows = jnp.where(core == 0, jnp.concatenate([stream, other]), jnp.concatenate([other, stream]))

    large, small = call(
        prepare_kernel,
        [((2 * HID + 2 * MIX, LANE), BF16), ((HID + 2 * TAIL, LANE), BF16)],
        [],
        [
            gate_weight.T,
            up_weight.T,
            query_weight.T,
            key_weight.T,
            value_weight,
            outgate_weight,
            down_weight,
            out_weight,
        ],
        [pltpu.VMEM((LANE, DV), BF16), pltpu.VMEM((LANE, DV), BF16), pltpu.SemaphoreType.DMA((9,))],
        space=pltpu.HBM,
    )
    flat_ffn, flat_mix, flat_rest = [], [], []
    for shard, orders, units in ((small, SMALL, HID), (large, LARGE, 2 * HID)):
        planes = gathered_planes(shard, orders)
        size = (4, 4, (shard.shape[0] - units) // 2, LANE)
        half = ((2, 4, units, LANE), BF16)
        (low,) = call(divide_low_kernel, [half], [], planes[:2])
        high, mix, rest = call(divide_high_kernel, [half, (size, BF16), (size, BF16)], [], planes)
        flat_ffn = gathered_ring(low, high, last_of(orders)) + flat_ffn
        flat_mix = gathered_direct(mix, last_of(orders)) + flat_mix
        flat_rest = gathered_direct(rest, last_of(orders)) + flat_rest
    decay = jnp.concatenate(
        [decay_up.astype(F32), decay_bias[None, :], jnp.zeros((7, DK), F32)], axis=0
    )
    everyone = lax.all_gather(decay, "y", axis=0)
    everyone = jnp.concatenate([everyone, everyone], axis=0)
    ordered = lax.dynamic_slice_in_dim(everyone, lax.axis_index("y"), 4, 0)
    decay = jnp.moveaxis(ordered, 0, 1).reshape(40, HEADS * DK)

    rows, decay_rows, decay_bias_row = lax.optimization_barrier((rows, decay[:32].astype(BF16), decay[32:33]))
    large_p, small_p = flat_ffn[:8], flat_ffn[8:]
    near, part = call(
        ffn_early_kernel,
        [((4, 3, 4, 2 * HID, LANE), BF16), ((4, ROWS, 2 * HID), F32)],
        [place],
        [rows, *large_p[:4], *large_p[6:]],
        (),
        2_200_000_000,
    )
    part, far = call(
        ffn_late_kernel,
        [((ROWS, D), BF16), ((4, 4, 2 * HID, LANE), BF16)],
        [place],
        [rows, part, *large_p[4:6], *small_p],
        FFN_SCRATCH,
        2_200_000_000,
    )
    wide = ((ROWS, HEADS * DK), BF16)
    broad = ((ROWS, HEADS * DV), BF16)
    first, query, keys, values, ghi, glo, state = call(
        project_kernel,
        [((ROWS, D), BF16), wide, wide, broad, wide, wide, ((DV + 8, HEADS * DK), F32)],
        [place],
        [
            rows,
            part,
            swapped(part),
            norm_gain[0:1],
            decay_down.T,
            decay_rows,
            decay_bias_row,
            *flat_mix,
        ],
        [pltpu.VMEM((4, ROWS, MIX + TAIL), BF16), pltpu.VMEM((4, 4, MIX, LANE), BF16), pltpu.VMEM((4, 4, TAIL, LANE), BF16)],
        2_000_000_000,
    )
    earlier = [
        lax.ppermute(state, "y", [(i, i + back) for i in range(4 - back)]) for back in (1, 2, 3)
    ]
    (mixed,) = call(
        inside_kernel,
        [((ROWS, HEADS * DV), F32)],
        [],
        [query, keys, values, ghi, glo],
        [pltpu.VMEM((HEADS * ROWS, ROWS), F32)],
        4_000_000_000,
    )
    (part,) = call(
        output_kernel,
        [((ROWS, D), BF16)],
        [place],
        [mixed, query, ghi, glo, first, head_gain[None, :], *earlier, *flat_rest],
        [
            pltpu.VMEM((4, 4, 4, MIX, LANE), BF16),
            pltpu.VMEM((4, 4, 4, TAIL, LANE), BF16),
            pltpu.VMEM((4, ROWS, DV), BF16),
        ],
        1_000_000_000,
    )
    own, keep, give = call(
        ffn_second_kernel,
        [((128, D), BF16)] * 3,
        [place],
        [first, part, swapped(part), norm_gain[1:2], near, far, *small_p],
        [*FFN_SCRATCH, pltpu.VMEM((ROWS, D), BF16)],
        4_400_000_000,
    )
    (out,) = call(last_norm_kernel, [((128, D), BF16)], [], [own, keep, swapped(give), norm_gain[2:3]])
    return out


def solution(mesh):
    fine = Mesh(mesh.devices.reshape(2, 4, 4, 4, 2), ("r", "z", "x", "y", "c"))
    fs, tp = ("z", "x"), ("y", "c")
    in_specs = (
        P(("r", *fs, *tp), None),
        P(fs, tp),
        P(fs, tp),
        P(tp, fs),
        P(fs, tp),
        P(fs, tp),
        P(fs, tp),
        P(fs, tp),
        P(),
        P(None, tp),
        P(tp),
        P(),
        P(tp, fs),
        P(),
    )
    return jax.shard_map(on_device, mesh=fine, in_specs=in_specs, out_specs=P(("r", *fs, *tp), None), check_vma=False)
```
